512 devices in a mesh: fs: 32 (over z, core), tp: 16 (over y, x).
Axes of the slice: x: 4, y: 4, z: 16, core: 2. Of those that a mesh axis runs over, the one named last changes fastest.
Arguments:
- tokens: bfloat16 [4096, 2048], P('fs'), may hold values from -6 to 6
- experts: int32 [4096, 4], P('fs'), may hold values from 0 to 31, all different within a row; in each aligned block of 128 rows (0 to 127, 128 to 255, ...) at most 24 rows name the same one
- routing: float32 [4096, 4], P('fs'), may hold values from 0.05 to 0.6
- norm_gain: float32 [2048], replicated, may hold values from 0.1 to 1.9
- gate_master: float32 [32, 2048, 2048], P(None, 'fs', 'tp'), may hold values from -0.625 to 0.625
- linear_master: float32 [32, 2048, 2048], P(None, 'fs', 'tp'), may hold values from -0.625 to 0.625
- down_weight: bfloat16 [32, 2048, 2048], P('fs', None, 'tp'), may hold values from -0.013671875 to 0.013671875
Outputs:
- gate_out: bfloat16 [32, 2048, 2048], P('fs', None, 'tp')
- linear_out: bfloat16 [32, 2048, 2048], P('fs', None, 'tp')
- expert_mix: bfloat16 [4096, 2048], P('fs', 'tp')
The draws below stay inside these ranges and needn't reach their ends.
Inputs may be any that keep to these rules, and one draw needn't show every extreme that they name: Each row names 4 different experts; within the rows of one index of fs (aligned blocks of 128 rows) no expert is named by more than 24 rows, and in some blocks some expert is named by exactly 24; every expert is named somewhere.
All inputs are finite; a program needn't handle non-finite values.
Results may differ from the reference program's by a relative error of at most 0.023.
Values may be sent and summed in bfloat16 or wider, within the bound.
A program may use at most 64 MiB of HBM per device.

```python
import math
import jax
import jax.numpy as jnp
import numpy as np
from jax import lax

D = 2048
DE = 2048
TOP = 4
TOK_DEV = 128
EXPERTS = 32
HID_DEV = 128
CAP = 24
TOKENS = 4096
N_TP = 16


def levels(key, dims, shards, smallest, largest):
    level = 1.0
    for position, blocks in shards:
        draws = jax.random.uniform(jax.random.fold_in(jax.random.fold_in(key, 6), position), (blocks,), jnp.float32, smallest / len(shards), largest / len(shards))
        level = level * jnp.repeat(jnp.exp(draws), dims[position] // blocks).reshape((-1,) + (1,) * (len(dims) - 1 - position))
    return level


def assign_block(own_key, own, number, rows, count, top, most, lean):
    sequence = jax.random.permutation(own_key, count)
    packed, usual = shares(count, rows * top, most, lean, True), shares(count, rows * top, most, lean, False)
    places = jnp.arange(count)

    def named(tallies, offset_by):
        used = int((tallies > 0).sum())
        fixed = max(1, used // 4)
        moved = fixed + (places - fixed + offset_by * (used - fixed)) % max(1, count - fixed)
        return jnp.zeros((count,), jnp.int32).at[sequence[jnp.where(places < fixed, places, moved)]].set(jnp.asarray(tallies, jnp.int32))

    tallies = jnp.where(number % 4 == 0, named(packed, number // 4), named(usual, number - number // 4 - 1))
    mixed = jax.random.permutation(jax.random.fold_in(own, 3), count)
    donor, sink = mixed[0:count // 2 * 2:2], mixed[1:count // 2 * 2:2]
    room = jnp.minimum(tallies[donor] - 1, most - tallies[sink]) // 2
    room = jnp.where((donor == sequence[0]) | (sink == sequence[0]) | (tallies[sink] == 0), 0, jnp.maximum(room, 0))
    moved = jax.random.randint(jax.random.fold_in(own, 4), (count // 2,), 0, 1 << 20) % (room + 1)
    tallies = tallies.at[donor].add(-moved).at[sink].add(moved)
    labels = jnp.searchsorted(jnp.cumsum(tallies), jnp.arange(rows * top), side="right").astype(jnp.int32)
    listing = labels.reshape(top, rows).T
    listing = listing[jax.random.permutation(jax.random.fold_in(own, 1), rows)]
    offset_by = jax.random.randint(jax.random.fold_in(own, 2), (rows, 1), 0, top)
    return jnp.take_along_axis(listing, (jnp.arange(top)[None, :] + offset_by) % top, axis=1)


def shares(number_of, total, limit, lean, full):
    loads = [(1 << 20) // math.isqrt(rank ** lean) + 1 for rank in range(1, number_of + 1)]
    largest = limit if full else min(limit, max(-(-total // number_of), total * loads[0] // sum(loads)))
    least = 1 if total - largest >= number_of - 1 else 0
    given, surplus = [largest] + [least] * (number_of - 1), total - largest - least * (number_of - 1)
    while surplus > 0:
        movable = [i for i in range(1, number_of) if given[i] < largest] or [i for i in range(1, number_of) if given[i] < limit]
        mass, budget = sum([loads[i] for i in movable]), surplus
        for i in movable:
            extra = min(limit - given[i], max(1, budget * loads[i] // mass), surplus)
            given[i] = given[i] + extra
            surplus = surplus - extra
    return np.array(given)


def centred(stream_key, shape, scale, bound, shards=(), kind=jnp.bfloat16):
    loudness = levels(stream_key, shape, shards, -0.22, 0.18) if shards else 1.0
    entries = jax.random.normal(stream_key, shape, jnp.float32) * scale * loudness
    return jnp.minimum(jnp.maximum(entries, -bound), bound).astype(kind)


def setup_inputs(seed: int = 0) -> dict:
    key_list = jax.random.split(jax.random.key(seed), 8)
    tokens = centred(key_list[0], (TOKENS, D), 1.0, 6.0, ((0, 32),))
    experts_keys = jax.random.split(jax.random.fold_in(key_list[1], 1), TOKENS // TOK_DEV)
    experts_turns = jax.random.permutation(jax.random.fold_in(key_list[1], 3), TOKENS // TOK_DEV)
    experts = jax.vmap(lambda own, number: assign_block(jax.random.fold_in(key_list[1], 2), own, number, TOK_DEV, EXPERTS, TOP, CAP, 0))(experts_keys, experts_turns).reshape((TOKENS, TOP))
    routing = jnp.clip(0.05 + 0.55 * jax.random.uniform(key_list[2], (TOKENS, TOP), jnp.float32) ** levels(key_list[2], (TOKENS, TOP), ((0, 32),), -0.2, 0.2), 0.05, 0.6)
    norm_gain = jnp.clip(1.0 + 0.18 * jax.random.normal(key_list[3], (D,), jnp.float32), 0.1, 1.9)
    gate_master = centred(key_list[4], (EXPERTS, D, DE), (D // 25) ** -0.5, 0.625, ((1, 32), (2, 16)), jnp.float32)
    linear_master = centred(key_list[5], (EXPERTS, D, DE), (D // 25) ** -0.5, 0.625, ((1, 32), (2, 16)), jnp.float32)
    down_weight = centred(key_list[6], (EXPERTS, D, DE), (DE * 100) ** -0.5, 0.013671875, ((0, 32), (2, 16)))
    return dict(tokens=tokens, experts=experts, routing=routing, norm_gain=norm_gain, gate_master=gate_master, linear_master=linear_master, down_weight=down_weight)


clamp_limit = 7.0
gate_slope = 1.702


def reference(tokens, experts, routing, norm_gain, gate_master, linear_master, down_weight):
    gain_col = norm_gain[None, :, None]
    gate_out = (gate_master * gain_col).astype(jnp.bfloat16)
    linear_out = (linear_master * gain_col).astype(jnp.bfloat16)
    flat_ids = experts.reshape(-1)
    owner = jnp.arange(TOKENS * TOP, dtype=jnp.int32) // TOP
    weights = routing.reshape(-1)
    span_rows = CAP * EXPERTS

    def one_expert(running, expert_id):
        pick_order = jnp.argsort((flat_ids != expert_id).astype(jnp.int32), stable=True)[:span_rows]
        in_use = flat_ids[pick_order] == expert_id
        row_owner = owner[pick_order]
        row_data = tokens[row_owner]
        pre_gate = jnp.dot(row_data, gate_out[expert_id], preferred_element_type=jnp.float32)
        pre_linear = jnp.dot(row_data, linear_out[expert_id], preferred_element_type=jnp.float32)
        clamped = jnp.minimum(pre_gate, clamp_limit)
        active = (clamped * jax.nn.sigmoid(gate_slope * clamped)
                  * (jnp.clip(pre_linear, -clamp_limit, clamp_limit) + 1.0)).astype(jnp.bfloat16)
        blocks = active.astype(jnp.float32).reshape(span_rows, N_TP, HID_DEV)
        down_blocks = down_weight[expert_id].astype(jnp.float32).reshape(D, N_TP, HID_DEV)
        block_part = jnp.einsum("rbh,dbh->rbd", blocks, down_blocks)
        rounded = lax.optimization_barrier(block_part.astype(jnp.bfloat16)).astype(jnp.float32)
        total = jnp.sum(rounded, axis=1)
        scale_rows = jnp.where(in_use, weights[pick_order], jnp.float32(0.0))
        running = running.at[row_owner].add(total * scale_rows[:, None])
        return running, None

    start = jnp.zeros((TOKENS, D), jnp.float32)
    final, _ = lax.scan(one_expert, start, jnp.arange(EXPERTS, dtype=jnp.int32))
    return (gate_out, linear_out, final.astype(jnp.bfloat16))
```

```python
import jax
import jax.numpy as jnp
from jax import lax
from jax.sharding import PartitionSpec as P

clamp_limit = 7.0
gate_slope = 1.702
BF = jnp.bfloat16
F32 = jnp.float32


def dispatch_table(experts, routing, expert_count, capacity):
    tok = experts.shape[0]
    ids = experts.T
    names = jnp.arange(expert_count, dtype=jnp.int32)[:, None]
    chosen = jnp.zeros((expert_count, tok), F32)
    weight = jnp.zeros((expert_count, tok), F32)
    rt = routing.T
    for k in range(ids.shape[0]):
        hit = ids[k][None, :] == names
        chosen = chosen + jnp.where(hit, 1.0, 0.0)
        weight = weight + jnp.where(hit, rt[k][None, :], 0.0)
    before = (
        lax.broadcasted_iota(jnp.int32, (tok, tok), 0)
        < lax.broadcasted_iota(jnp.int32, (tok, tok), 1)
    ).astype(BF)
    rank = jnp.dot(chosen.astype(BF), before, preferred_element_type=F32)
    slot = jnp.where(chosen > 0, rank, -1.0)
    places = jnp.arange(capacity, dtype=jnp.int32).astype(F32)
    table = slot[:, None, :] == places[None, :, None]
    return table, weight


def on_device(tokens, experts, routing, norm_gain, gate_master, linear_master, down_weight):
    tok, top = experts.shape
    ecount, stripe, hid = gate_master.shape
    width = tokens.shape[1]
    n_tp = lax.axis_size("tp")
    fcols = width // n_tp
    cap = 3 * tok * top // (2 * ecount)
    gain = lax.dynamic_slice_in_dim(norm_gain, lax.axis_index("fs") * stripe, stripe)[None, :, None]
    both = jnp.concatenate(
        [(gate_master * gain).astype(BF), (linear_master * gain).astype(BF)], axis=2
    )
    filled = lax.all_to_all(both, "fs", split_axis=0, concat_axis=1, tiled=True)
    gate_out, linear_out = filled[:, :, :hid], filled[:, :, hid:]
    table, weight = dispatch_table(experts, routing, ecount, cap)
    pick = jnp.where(table, 1.0, 0.0).astype(BF).reshape(ecount * cap, tok)
    mine = lax.dynamic_slice_in_dim(tokens, lax.axis_index("tp") * fcols, fcols, axis=1)
    send = jnp.dot(pick, mine, preferred_element_type=F32).astype(BF)
    rows = lax.all_to_all(
        send.reshape(ecount, cap, fcols), "fs", split_axis=0, concat_axis=0, tiled=True
    )
    tokens_all = lax.all_gather(rows.reshape(ecount * cap, fcols), "tp", axis=0)
    down_mine = lax.all_to_all(
        down_weight[0].reshape(n_tp, fcols, hid), "tp", split_axis=0, concat_axis=0, tiled=True
    )
    dims = (((0, 2), (0, 1)), ((), ()))
    pre_gate = lax.dot_general(
        tokens_all, gate_out[0].reshape(n_tp, fcols, hid), dims, preferred_element_type=F32
    )
    pre_linear = lax.dot_general(
        tokens_all, linear_out[0].reshape(n_tp, fcols, hid), dims, preferred_element_type=F32
    )
    clamped = jnp.minimum(pre_gate, clamp_limit)
    active = (
        clamped
        * jax.nn.sigmoid(gate_slope * clamped)
        * (jnp.clip(pre_linear, -clamp_limit, clamp_limit) + 1.0)
    ).astype(BF)
    active_all = lax.all_gather(active, "tp", axis=0)
    summed = lax.dot_general(
        active_all, down_mine, (((0, 2), (0, 2)), ((), ())), preferred_element_type=F32
    )
    back = lax.all_to_all(
        summed.astype(BF).reshape(ecount, cap, fcols), "fs", split_axis=0, concat_axis=0, tiled=True
    ).reshape(ecount * cap, fcols)
    mixer = jnp.where(table, weight[:, None, :], 0.0).reshape(ecount * cap, tok)
    high = mixer.astype(BF)
    low = (mixer - high.astype(F32)).astype(BF)
    cdims = (((0,), (0,)), ((), ()))
    mix = lax.dot_general(high, back, cdims, preferred_element_type=F32) + lax.dot_general(
        low, back, cdims, preferred_element_type=F32
    )
    return gate_out, linear_out, mix.astype(BF)


def solution(mesh):
    return jax.shard_map(
        on_device,
        mesh=mesh,
        in_specs=(
            P("fs", None),
            P("fs", None),
            P("fs", None),
            P(),
            P(None, "fs", "tp"),
            P(None, "fs", "tp"),
            P("fs", None, "tp"),
        ),
        out_specs=(P("fs", None, "tp"), P("fs", None, "tp"), P("fs", "tp")),
        check_vma=False,
    )
```

```python
import functools

import jax
import jax.numpy as jnp
from jax import lax
from jax.experimental import pallas as pl
from jax.experimental.pallas import tpu as pltpu
from jax.sharding import PartitionSpec as P

clamp_limit = 7.0
gate_slope = 1.702
BF = jnp.bfloat16
F32 = jnp.float32
MESH = pl.DeviceIdType.MESH
SIDE = 4


def remote(src, dst, send_sem, recv_sem, device):
    return pltpu.make_async_remote_copy(
        src_ref=src,
        dst_ref=dst,
        send_sem=send_sem,
        recv_sem=recv_sem,
        device_id=device,
        device_id_type=MESH,
    )


class Torus:
    def __init__(self, grid, send_sems, recv_sems, t):
        self.grid, self.send_sems, self.recv_sems = grid, send_sems, recv_sems
        self.y, self.x = t // SIDE, t % SIDE
        tiles = grid.shape[1]
        self.half, self.quarter = tiles // 2, tiles // 4
        self.sent = []

    def at(self, h, a, b):
        dx, dy = (a, b) if h == 0 else (b, a)
        return ((self.y + dy + SIDE) % SIDE) * SIDE + (self.x + dx + SIDE) % SIDE

    def copy(self, h, slot, a, b, part, to):
        start = h * self.half + (self.quarter if part == 1 else 0)
        size = self.half if part is None else self.quarter
        ref = self.grid.at[self.at(h, a, b), pl.ds(start, size)]
        k = h * 20 + slot
        return remote(ref, ref, self.send_sems.at[k], self.recv_sems.at[k], {"tp": self.at(h, *to)})

    def send(self, h, slot, a, b, part, to):
        c = self.copy(h, slot, a, b, part, to)
        c.start()
        self.sent.append(c)

    def recv(self, h, slot, a, b, part):
        self.copy(h, slot, a, b, part, (1, 0)).wait_recv()

    def own(self):
        for h in (0, 1):
            self.send(h, 0, 0, 0, None, (1, 0))
            self.send(h, 1, 0, 0, None, (-1, 0))
            self.column(h, 0, 0)

    def column(self, h, i, a):
        self.send(h, 4 + 4 * i, a, 0, None, (0, 1))
        self.send(h, 5 + 4 * i, a, 0, None, (0, -1))

    def turn(self, h, i, a):
        self.recv(h, 4 + 4 * i, a, -1, None)
        self.send(h, 6 + 4 * i, a, -1, 0, (0, 1))
        self.recv(h, 5 + 4 * i, a, 1, None)
        self.send(h, 7 + 4 * i, a, 1, 1, (0, -1))

    def rest(self):
        for h in (0, 1):
            self.recv(h, 0, -1, 0, None)
            self.send(h, 2, -1, 0, 0, (1, 0))
            self.column(h, 1, -1)
            self.recv(h, 1, 1, 0, None)
            self.send(h, 3, 1, 0, 1, (-1, 0))
            self.column(h, 2, 1)
        for h in (0, 1):
            self.turn(h, 0, 0)
        for h in (0, 1):
            self.recv(h, 2, 2, 0, 0)
            self.recv(h, 3, 2, 0, 1)
            self.column(h, 3, 2)
        for h in (0, 1):
            self.turn(h, 1, -1)
            self.turn(h, 2, 1)
        for h in (0, 1):
            self.turn(h, 3, 2)
        for h in (0, 1):
            for i, a in enumerate((0, -1, 1, 2)):
                self.recv(h, 6 + 4 * i, a, 2, 0)
                self.recv(h, 7 + 4 * i, a, 2, 1)

    def drain(self):
        for c in self.sent:
            c.wait_send()


def kernel(
    n_fs,
    n_tp,
    experts_ref,
    routing_ref,
    gain_ref,
    tokens_hbm,
    gate_hbm,
    linear_hbm,
    down_hbm,
    gate_out,
    linear_out,
    mix_out,
    gate_v,
    linear_v,
    tok_v,
    down_v,
    w_send,
    w_recv,
    t_send,
    t_grid,
    a_grid,
    d_recv,
    r_send,
    r_recv,
    slot_v,
    weight_v,
    pick_v,
    mixer_v,
    high_v,
    low_v,
    acc,
    acc2,
    local_sems,
    t_ssem,
    t_rsem,
    w_ssem,
    w_rsem,
    r_ssem,
    r_rsem,
    d_ssem,
    d_rsem,
    tg_ssem,
    tg_rsem,
    ag_ssem,
    ag_rsem,
):
    f, t = lax.axis_index("fs"), lax.axis_index("tp")
    n_z = n_fs // 2
    z, c = f // 2, f % 2
    stripe, hid = gate_v.shape[1], gate_v.shape[2]
    fcols = tok_v.shape[1]
    tok = tok_v.shape[0]
    tiles = t_grid.shape[1]
    rows = tiles * 8
    per = tiles // n_fs
    cap = per * 8

    loads = [
        pltpu.make_async_copy(
            tokens_hbm.at[:, pl.ds(pl.multiple_of(t * fcols, 128), fcols)], tok_v, local_sems.at[0]
        ),
        pltpu.make_async_copy(gate_hbm, gate_v, local_sems.at[1]),
        pltpu.make_async_copy(linear_hbm, linear_v, local_sems.at[2]),
        pltpu.make_async_copy(down_hbm, down_v, local_sems.at[3]),
    ]
    for load in loads:
        load.start()

    barrier = pltpu.get_barrier_semaphore()

    @pl.loop(1, n_fs)
    def _(k):
        pl.semaphore_signal(
            barrier, inc=1, device_id={"fs": (f + k) % n_fs}, device_id_type=MESH
        )

    @pl.loop(1, n_tp)
    def _(k):
        pl.semaphore_signal(
            barrier, inc=1, device_id={"tp": (t + k) % n_tp}, device_id_type=MESH
        )

    names = lax.broadcasted_iota(jnp.int32, (n_fs, tok), 0)
    chosen = jnp.zeros((n_fs, tok), F32)
    weight = jnp.zeros((n_fs, tok), F32)
    for k in range(experts_ref.shape[0]):
        hit = experts_ref[k : k + 1, :] == names
        chosen = chosen + jnp.where(hit, 1.0, 0.0)
        weight = weight + jnp.where(hit, routing_ref[k : k + 1, :], 0.0)
    before = jnp.where(
        lax.broadcasted_iota(jnp.int32, (tok, tok), 0)
        < lax.broadcasted_iota(jnp.int32, (tok, tok), 1),
        1.0,
        0.0,
    ).astype(BF)
    rank = jnp.dot(chosen.astype(BF), before, preferred_element_type=F32)
    slot_v[...] = jnp.where(chosen > 0.0, rank, -1.0)
    weight_v[...] = weight
    places = lax.broadcasted_iota(jnp.int32, (cap, tok), 0).astype(F32)

    @pl.loop(0, n_fs)
    def _(e):
        hit = slot_v[pl.ds(e, 1), :] == places
        at = pl.ds(pl.multiple_of(e * cap, 8), cap)
        pick_v[at, :] = jnp.where(hit, 1.0, 0.0)
        mixer_v[at, :] = jnp.where(hit, weight_v[pl.ds(e, 1), :], 0.0)

    loads[0].wait()
    sent = jnp.dot(pick_v[...].astype(BF), tok_v[...], preferred_element_type=F32)
    t_send[...] = sent.astype(BF).reshape(tiles, 8, fcols)

    here = lax.broadcasted_iota(jnp.int32, (stripe, hid), 0) + (f * stripe) % hid
    lane = lax.broadcasted_iota(jnp.int32, (stripe, hid), 1)
    picked = jnp.where(here == lane, gain_ref[pl.ds((f * stripe) // hid, 1), :], 0.0)
    column = jnp.sum(picked, axis=1, keepdims=True)
    loads[1].wait()
    loads[2].wait()

    @pl.loop(0, n_fs)
    def _(e):
        w_send[e, :, 0:hid] = (gate_v[e] * column).astype(BF)
        w_send[e, :, hid : 2 * hid] = (linear_v[e] * column).astype(BF)

    loads[3].wait()
    pl.semaphore_wait(barrier, n_fs + n_tp - 2)

    def tile_span(i):
        return pl.ds(i * per, per)

    def peer(dz, dc):
        return ((z + dz) % n_z) * 2 + (c + dc) % 2

    def source(dz, dc):
        return ((z - dz + n_z) % n_z) * 2 + (c + dc) % 2

    def turn(k):
        return (n_z // 2 + (1 - 2 * (k % 2)) * ((k + 1) // 2)) % n_z

    def tokens_copy(dz, dc, to, slot):
        i = dz * 2 + dc
        return remote(
            t_send.at[tile_span(to)],
            t_grid.at[t, tile_span(slot)],
            t_ssem.at[i],
            t_rsem.at[i],
            {"fs": to},
        )

    def weights_copy(dz, dc, to, slot):
        i = dz * 2 + dc
        return remote(w_send.at[to], w_recv.at[slot], w_ssem.at[i], w_rsem.at[i], {"fs": to})

    def return_copy(dz, dc, to, slot):
        i = dz * 2 + dc
        return remote(
            r_send.at[tile_span(to)],
            r_recv.at[tile_span(slot)],
            r_ssem.at[i],
            r_rsem.at[i],
            {"fs": to},
        )

    def start_all(copy):
        @pl.loop(0, n_z - 1)
        def _(k):
            dz = turn(k)
            for dc in (0, 1):
                copy(dz, dc, peer(dz, dc), f).start()

        copy(0, 1, peer(0, 1), f).start()

    def recv_all(copy):
        copy(0, 1, peer(0, 1), source(0, 1)).wait_recv()

        @pl.loop(0, n_z - 1)
        def _(k):
            dz = turn(k)
            for dc in (0, 1):
                copy(dz, dc, peer(dz, dc), source(dz, dc)).wait_recv()

    def drain_all(copy):
        copy(0, 1, peer(0, 1), f).wait_send()

        @pl.loop(0, n_z - 1)
        def _(k):
            dz = turn(k)
            for dc in (0, 1):
                copy(dz, dc, peer(dz, dc), f).wait_send()

    def down_copy(k, slot):
        to = (t + k) % n_tp
        return remote(
            down_v.at[to], d_recv.at[slot], d_ssem.at[k], d_rsem.at[k], {"tp": to}
        )

    start_all(tokens_copy)
    start_all(weights_copy)

    @pl.loop(1, n_tp)
    def _(k):
        down_copy(k, t).start()

    t_grid[t, tile_span(f)] = t_send[tile_span(f)]
    w_recv[f] = w_send[f]
    d_recv[t] = down_v[t]
    for j in range(rows // 128):
        at = slice(j * 128, (j + 1) * 128)
        turned = mixer_v[at, :].T
        high = turned.astype(BF)
        high_v[:, at] = high
        low_v[:, at] = (turned - high.astype(F32)).astype(BF)
    acc[...] = jnp.zeros_like(acc)

    recv_all(tokens_copy)
    tg = Torus(t_grid, tg_ssem, tg_rsem, t)
    tg.own()
    tg.rest()

    ratio = (2 * stripe) // fcols

    def multiply(chip):
        for j in range(ratio):
            block = chip * ratio + j
            lhs = t_grid[block].reshape(rows, fcols)
            if ratio == 1:
                rhs = w_recv[pl.ds(chip * 2, 2)].reshape(fcols, 2 * hid)
            else:
                rhs = w_recv[chip * 2 + j // (ratio // 2), (j % (ratio // 2)) * fcols :][:fcols]
            acc[...] += jnp.dot(lhs, rhs, preferred_element_type=F32)

    weights_copy(0, 1, peer(0, 1), source(0, 1)).wait_recv()
    multiply(z)

    @pl.loop(0, n_z - 1)
    def _(k):
        dz = turn(k)
        for dc in (0, 1):
            weights_copy(dz, dc, peer(dz, dc), source(dz, dc)).wait_recv()
        multiply((z - dz + n_z) % n_z)

    stores = [
        pltpu.make_async_copy(w_recv.at[:, :, pl.ds(0, hid)], gate_out, local_sems.at[4]),
        pltpu.make_async_copy(w_recv.at[:, :, pl.ds(hid, hid)], linear_out, local_sems.at[5]),
    ]
    for store in stores:
        store.start()

    clamped = jnp.minimum(acc[:, 0:hid], clamp_limit)
    linear = jnp.clip(acc[:, hid : 2 * hid], -clamp_limit, clamp_limit)
    active = clamped * jax.nn.sigmoid(gate_slope * clamped) * (linear + 1.0)
    a_grid[t] = active.astype(BF).reshape(tiles, 8, hid)

    ag = Torus(a_grid, ag_ssem, ag_rsem, t)
    ag.own()
    acc2[...] = jnp.zeros_like(acc2)

    @pl.loop(1, n_tp)
    def _(k):
        down_copy(k, (t - k + n_tp) % n_tp).wait_recv()

    ag.rest()

    @pl.loop(0, n_tp)
    def _(b):
        acc2[...] += lax.dot_general(
            a_grid[b].reshape(rows, hid),
            d_recv[b],
            (((1,), (1,)), ((), ())),
            preferred_element_type=F32,
        )

    r_send[...] = acc2[...].astype(BF).reshape(tiles, 8, fcols)
    start_all(return_copy)
    r_recv[tile_span(f)] = r_send[tile_span(f)]
    drain_all(tokens_copy)
    drain_all(weights_copy)

    @pl.loop(1, n_tp)
    def _(k):
        down_copy(k, t).wait_send()

    tg.drain()
    ag.drain()
    for store in stores:
        store.wait()
    recv_all(return_copy)
    back = r_recv[...].reshape(rows, fcols)
    mix = jnp.dot(high_v[...], back, preferred_element_type=F32) + jnp.dot(
        low_v[...], back, preferred_element_type=F32
    )
    mix_out[...] = mix.astype(BF)
    drain_all(return_copy)


def on_device(n_fs, n_tp, tokens, experts, routing, gain, gate_master, linear_master, down_weight):
    tok, top = experts.shape
    ecount, stripe, hid = gate_master.shape
    width = tokens.shape[1]
    fcols = width // n_tp
    cap = 3 * tok * top // (2 * ecount)
    tiles = ecount * cap // 8
    rows = ecount * cap
    vmem, any_space = pl.BlockSpec(memory_space=pltpu.VMEM), pl.BlockSpec(memory_space=pl.ANY)
    dma = pltpu.SemaphoreType.DMA
    gate_out, linear_out, mix = pl.pallas_call(
        functools.partial(kernel, n_fs, n_tp),
        out_shape=(
            jax.ShapeDtypeStruct((ecount, stripe, hid), BF),
            jax.ShapeDtypeStruct((ecount, stripe, hid), BF),
            jax.ShapeDtypeStruct((tok, fcols), BF),
        ),
        in_specs=[vmem] * 3 + [any_space] * 4,
        out_specs=(any_space, any_space, vmem),
        scratch_shapes=[
            pltpu.VMEM((ecount, stripe, hid), F32),
            pltpu.VMEM((ecount, stripe, hid), F32),
            pltpu.VMEM((tok, fcols), BF),
            pltpu.VMEM((n_tp, fcols, hid), BF),
            pltpu.VMEM((ecount, stripe, 2 * hid), BF),
            pltpu.VMEM((ecount, stripe, 2 * hid), BF),
            pltpu.VMEM((tiles, 8, fcols), BF),
            pltpu.VMEM((n_tp, tiles, 8, fcols), BF),
            pltpu.VMEM((n_tp, tiles, 8, hid), BF),
            pltpu.VMEM((n_tp, fcols, hid), BF),
            pltpu.VMEM((tiles, 8, fcols), BF),
            pltpu.VMEM((tiles, 8, fcols), BF),
            pltpu.VMEM((ecount, tok), F32),
            pltpu.VMEM((ecount, tok), F32),
            pltpu.VMEM((rows, tok), F32),
            pltpu.VMEM((rows, tok), F32),
            pltpu.VMEM((tok, rows), BF),
            pltpu.VMEM((tok, rows), BF),
            pltpu.VMEM((rows, 2 * hid), F32),
            pltpu.VMEM((rows, fcols), F32),
            dma((6,)),
            dma((n_fs,)),
            dma((n_fs,)),
            dma((n_fs,)),
            dma((n_fs,)),
            dma((n_fs,)),
            dma((n_fs,)),
            dma((n_tp,)),
            dma((n_tp,)),
            dma((40,)),
            dma((40,)),
            dma((40,)),
            dma((40,)),
        ],
        compiler_params=pltpu.CompilerParams(
            collective_id=0, has_side_effects=True, vmem_limit_bytes=48 * 1024 * 1024
        ),
    )(
        experts.T,
        routing.T,
        gain.reshape(width // hid, hid),
        tokens,
        gate_master,
        linear_master,
        down_weight.reshape(n_tp, fcols, hid),
    )
    shape = (1, width, hid)
    return gate_out.reshape(shape), linear_out.reshape(shape), mix


def solution(mesh):
    n_fs, n_tp = mesh.shape["fs"], mesh.shape["tp"]
    return jax.shard_map(
        functools.partial(on_device, n_fs, n_tp),
        mesh=mesh,
        in_specs=(
            P("fs", None),
            P("fs", None),
            P("fs", None),
            P(),
            P(None, "fs", "tp"),
            P(None, "fs", "tp"),
            P("fs", None, "tp"),
        ),
        out_specs=(P("fs", None, "tp"), P("fs", None, "tp"), P("fs", "tp")),
        check_vma=False,
    )
```

```python
import functools

import jax
import jax.numpy as jnp
from jax import lax
from jax.experimental import pallas as pl
from jax.experimental.pallas import tpu as pltpu
from jax.sharding import PartitionSpec as P

clamp_limit = 7.0
gate_slope = 1.702
BF = jnp.bfloat16
F32 = jnp.float32
MESH = pl.DeviceIdType.MESH
SIDE = 4


def remote(src, dst, send_sem, recv_sem, device):
    return pltpu.make_async_remote_copy(
        src_ref=src,
        dst_ref=dst,
        send_sem=send_sem,
        recv_sem=recv_sem,
        device_id=device,
        device_id_type=MESH,
    )


class Torus:
    def __init__(self, grid, send_sems, recv_sems, t):
        self.grid, self.send_sems, self.recv_sems = grid, send_sems, recv_sems
        self.y, self.x = t // SIDE, t % SIDE
        tiles = grid.shape[1]
        self.half, self.quarter = tiles // 2, tiles // 4
        self.sent = []

    def at(self, h, a, b):
        dx, dy = (a, b) if h == 0 else (b, a)
        return ((self.y + dy + SIDE) % SIDE) * SIDE + (self.x + dx + SIDE) % SIDE

    def copy(self, h, slot, a, b, part, to):
        start = h * self.half + (self.quarter if part == 1 else 0)
        size = self.half if part is None else self.quarter
        ref = self.grid.at[self.at(h, a, b), pl.ds(start, size)]
        k = h * 20 + slot
        return remote(ref, ref, self.send_sems.at[k], self.recv_sems.at[k], {"tp": self.at(h, *to)})

    def send(self, h, slot, a, b, part, to):
        c = self.copy(h, slot, a, b, part, to)
        c.start()
        self.sent.append(c)

    def recv(self, h, slot, a, b, part):
        self.copy(h, slot, a, b, part, (1, 0)).wait_recv()

    def own(self):
        for h in (0, 1):
            self.send(h, 0, 0, 0, None, (1, 0))
            self.send(h, 1, 0, 0, None, (-1, 0))
            self.column(h, 0, 0)

    def column(self, h, i, a):
        self.send(h, 4 + 4 * i, a, 0, None, (0, 1))
        self.send(h, 5 + 4 * i, a, 0, None, (0, -1))

    def turn(self, h, i, a):
        self.recv(h, 4 + 4 * i, a, -1, None)
        self.send(h, 6 + 4 * i, a, -1, 0, (0, 1))
        self.recv(h, 5 + 4 * i, a, 1, None)
        self.send(h, 7 + 4 * i, a, 1, 1, (0, -1))

    def rest(self):
        for h in (0, 1):
            self.recv(h, 0, -1, 0, None)
            self.send(h, 2, -1, 0, 0, (1, 0))
            self.column(h, 1, -1)
            self.recv(h, 1, 1, 0, None)
            self.send(h, 3, 1, 0, 1, (-1, 0))
            self.column(h, 2, 1)
        for h in (0, 1):
            self.turn(h, 0, 0)
        for h in (0, 1):
            self.recv(h, 2, 2, 0, 0)
            self.recv(h, 3, 2, 0, 1)
            self.column(h, 3, 2)
        for h in (0, 1):
            self.turn(h, 1, -1)
            self.turn(h, 2, 1)
        for h in (0, 1):
            self.turn(h, 3, 2)
        for h in (0, 1):
            for i, a in enumerate((0, -1, 1, 2)):
                self.recv(h, 6 + 4 * i, a, 2, 0)
                self.recv(h, 7 + 4 * i, a, 2, 1)

    def drain(self):
        for c in self.sent:
            c.wait_send()


class Ring:
    def __init__(self, ref_of, device_of, send_sems, recv_sems, pos):
        self.ref_of, self.device_of, self.pos = ref_of, device_of, pos
        self.send_sems, self.recv_sems, self.sent = send_sems, recv_sems, []

    def at(self, step):
        return (self.pos + step + SIDE) % SIDE

    def copy(self, item, slot, step, part, to):
        ref = self.ref_of(self.at(step), item, part)
        k = item * 4 + slot
        return remote(
            ref, ref, self.send_sems.at[k], self.recv_sems.at[k], self.device_of(self.at(to))
        )

    def send(self, item, slot, step, part, to):
        c = self.copy(item, slot, step, part, to)
        c.start()
        self.sent.append(c)

    def first(self, item):
        self.send(item, 0, 0, None, 1)
        self.send(item, 1, 0, None, -1)

    def second(self, item):
        self.copy(item, 0, -1, None, 1).wait_recv()
        self.send(item, 2, -1, 0, 1)
        self.copy(item, 1, 1, None, 1).wait_recv()
        self.send(item, 3, 1, 1, -1)

    def last(self, item):
        self.copy(item, 2, 2, 0, 1).wait_recv()
        self.copy(item, 3, 2, 1, 1).wait_recv()

    def drain(self):
        for c in self.sent:
            c.wait_send()


def kernel(
    n_fs,
    n_tp,
    experts_hbm,
    routing_hbm,
    gain_hbm,
    tokens_hbm,
    gate_hbm,
    linear_hbm,
    down_hbm,
    gate_out,
    linear_out,
    mix_out,
    experts_ref,
    routing_ref,
    gain_ref,
    gate_v,
    linear_v,
    tok_v,
    down_v,
    w_send,
    w_recv,
    t_send,
    t_grid,
    a_send,
    a_grid,
    d_grid,
    r_send,
    r_recv,
    slot_v,
    weight_v,
    pick_v,
    mixer_v,
    high_v,
    low_v,
    acc,
    acc2,
    local_sems,
    t_ssem,
    t_rsem,
    w_ssem,
    w_rsem,
    r_ssem,
    r_rsem,
    dy_ssem,
    dy_rsem,
    dx_ssem,
    dx_rsem,
    tg_ssem,
    tg_rsem,
    ax_ssem,
    ax_rsem,
    ay_ssem,
    ay_rsem,
):
    f, t = lax.axis_index("fs"), lax.axis_index("tp")
    n_z = n_fs // 2
    z, c = f // 2, f % 2
    stripe, hid = gate_v.shape[1], gate_v.shape[2]
    fcols = tok_v.shape[1]
    tok = tok_v.shape[0]
    tiles = t_grid.shape[1]
    rows = tiles * 8
    per = tiles // n_fs
    cap = per * 8

    y, x = t // SIDE, t % SIDE
    loads = [
        pltpu.make_async_copy(
            tokens_hbm.at[:, pl.ds(pl.multiple_of(t * fcols, 128), fcols)], tok_v, local_sems.at[0]
        ),
        pltpu.make_async_copy(gate_hbm, gate_v, local_sems.at[1]),
        pltpu.make_async_copy(linear_hbm, linear_v, local_sems.at[2]),
        pltpu.make_async_copy(down_hbm, down_v, local_sems.at[3]),
        pltpu.make_async_copy(experts_hbm, experts_ref, local_sems.at[4]),
        pltpu.make_async_copy(routing_hbm, routing_ref, local_sems.at[5]),
        pltpu.make_async_copy(gain_hbm, gain_ref, local_sems.at[6]),
    ]
    for load in loads:
        load.start()

    barrier = pltpu.get_barrier_semaphore()

    @pl.loop(1, n_fs)
    def _(k):
        pl.semaphore_signal(
            barrier, inc=1, device_id={"fs": (f + k) % n_fs}, device_id_type=MESH
        )

    @pl.loop(1, n_tp)
    def _(k):
        pl.semaphore_signal(
            barrier, inc=1, device_id={"tp": (t + k) % n_tp}, device_id_type=MESH
        )

    loads[4].wait()
    loads[5].wait()
    names = lax.broadcasted_iota(jnp.int32, (n_fs, tok), 0)
    chosen = jnp.zeros((n_fs, tok), F32)
    weight = jnp.zeros((n_fs, tok), F32)
    for k in range(experts_ref.shape[0]):
        hit = experts_ref[k : k + 1, :] == names
        chosen = chosen + jnp.where(hit, 1.0, 0.0)
        weight = weight + jnp.where(hit, routing_ref[k : k + 1, :], 0.0)
    before = jnp.where(
        lax.broadcasted_iota(jnp.int32, (tok, tok), 0)
        < lax.broadcasted_iota(jnp.int32, (tok, tok), 1),
        1.0,
        0.0,
    ).astype(BF)
    rank = jnp.dot(chosen.astype(BF), before, preferred_element_type=F32)
    slot_v[...] = jnp.where(chosen > 0.0, rank, -1.0)
    weight_v[...] = weight
    places = lax.broadcasted_iota(jnp.int32, (cap, tok), 0).astype(F32)

    @pl.loop(0, n_fs)
    def _(e):
        hit = slot_v[pl.ds(e, 1), :] == places
        at = pl.ds(pl.multiple_of(e * cap, 8), cap)
        pick_v[at, :] = jnp.where(hit, 1.0, 0.0)
        mixer_v[at, :] = jnp.where(hit, weight_v[pl.ds(e, 1), :], 0.0)

    loads[0].wait()
    sent = jnp.dot(pick_v[...].astype(BF), tok_v[...], preferred_element_type=F32)
    t_send[...] = sent.astype(BF).reshape(tiles, 8, fcols)

    loads[6].wait()
    here = lax.broadcasted_iota(jnp.int32, (stripe, hid), 0) + (f * stripe) % hid
    lane = lax.broadcasted_iota(jnp.int32, (stripe, hid), 1)
    picked = jnp.where(here == lane, gain_ref[pl.ds((f * stripe) // hid, 1), :], 0.0)
    column = jnp.sum(picked, axis=1, keepdims=True)
    loads[1].wait()
    loads[2].wait()

    @pl.loop(0, n_fs)
    def _(e):
        w_send[e, :, 0:hid] = (gate_v[e] * column).astype(BF)
        w_send[e, :, hid : 2 * hid] = (linear_v[e] * column).astype(BF)

    loads[3].wait()
    pl.semaphore_wait(barrier, n_fs + n_tp - 2)

    def tile_span(i):
        return pl.ds(i * per, per)

    def peer(dz, dc):
        return ((z + dz) % n_z) * 2 + (c + dc) % 2

    def source(dz, dc):
        return ((z - dz + n_z) % n_z) * 2 + (c + dc) % 2

    def turn(k):
        return (n_z // 2 + (1 - 2 * (k % 2)) * ((k + 1) // 2)) % n_z

    def tokens_copy(dz, dc, to, slot):
        i = dz * 2 + dc
        return remote(
            t_send.at[tile_span(to)],
            t_grid.at[t, tile_span(slot)],
            t_ssem.at[i],
            t_rsem.at[i],
            {"fs": to},
        )

    def weights_copy(dz, dc, to, slot):
        i = dz * 2 + dc
        return remote(w_send.at[to], w_recv.at[slot], w_ssem.at[i], w_rsem.at[i], {"fs": to})

    def start_all(copy):
        @pl.loop(0, n_z - 1)
        def _(k):
            dz = turn(k)
            for dc in (0, 1):
                copy(dz, dc, peer(dz, dc), f).start()

        copy(0, 1, peer(0, 1), f).start()

    def recv_all(copy):
        copy(0, 1, peer(0, 1), source(0, 1)).wait_recv()

        @pl.loop(0, n_z - 1)
        def _(k):
            dz = turn(k)
            for dc in (0, 1):
                copy(dz, dc, peer(dz, dc), source(dz, dc)).wait_recv()

    def drain_all(copy):
        copy(0, 1, peer(0, 1), f).wait_send()

        @pl.loop(0, n_z - 1)
        def _(k):
            dz = turn(k)
            for dc in (0, 1):
                copy(dz, dc, peer(dz, dc), f).wait_send()

    def down_y(k, slot):
        to = (y + k) % SIDE
        return remote(
            down_v.at[to], d_grid.at[slot, x], dy_ssem.at[k], dy_rsem.at[k], {"tp": to * SIDE + x}
        )

    def down_ref(p, k, part):
        block = d_grid.at[(y - k + SIDE) % SIDE, p]
        half = d_grid.shape[2] // 2
        return block if part is None else block.at[pl.ds(part * half, half)]

    dx = Ring(down_ref, lambda p: {"tp": y * SIDE + p}, dx_ssem, dx_rsem, x)

    start_all(tokens_copy)
    start_all(weights_copy)

    for k in (1, 3, 2):
        down_y(k, y).start()
    d_grid[y, x] = down_v[y]
    dx.first(0)

    t_grid[t, tile_span(f)] = t_send[tile_span(f)]
    w_recv[f] = w_send[f]
    for j in range(rows // 128):
        at = slice(j * 128, (j + 1) * 128)
        turned = mixer_v[at, :].T
        high = turned.astype(BF)
        high_v[:, at] = high
        low_v[:, at] = (turned - high.astype(F32)).astype(BF)
    acc[...] = jnp.zeros_like(acc)

    for k in (1, 3, 2):
        down_y(k, (y - k + SIDE) % SIDE).wait_recv()
        dx.first(k)

    recv_all(tokens_copy)
    tg = Torus(t_grid, tg_ssem, tg_rsem, t)
    tg.own()
    for k in (0, 1, 3, 2):
        dx.second(k)
    tg.rest()

    ratio = (2 * stripe) // fcols

    def multiply(chip):
        for j in range(ratio):
            block = chip * ratio + j
            lhs = t_grid[block].reshape(rows, fcols)
            if ratio == 1:
                rhs = w_recv[pl.ds(chip * 2, 2)].reshape(fcols, 2 * hid)
            else:
                rhs = w_recv[chip * 2 + j // (ratio // 2), (j % (ratio // 2)) * fcols :][:fcols]
            acc[...] += jnp.dot(lhs, rhs, preferred_element_type=F32)

    weights_copy(0, 1, peer(0, 1), source(0, 1)).wait_recv()
    multiply(z)

    @pl.loop(0, n_z - 1)
    def _(k):
        dz = turn(k)
        for dc in (0, 1):
            weights_copy(dz, dc, peer(dz, dc), source(dz, dc)).wait_recv()
        multiply((z - dz + n_z) % n_z)

    stores = [
        pltpu.make_async_copy(w_recv.at[:, :, pl.ds(0, hid)], gate_out, local_sems.at[7]),
        pltpu.make_async_copy(w_recv.at[:, :, pl.ds(hid, hid)], linear_out, local_sems.at[8]),
    ]
    for store in stores:
        store.start()

    clamped = jnp.minimum(acc[:, 0:hid], clamp_limit)
    linear = jnp.clip(acc[:, hid : 2 * hid], -clamp_limit, clamp_limit)
    active = clamped * jax.nn.sigmoid(gate_slope * clamped) * (linear + 1.0)
    a_send[...] = active.astype(BF).reshape(a_send.shape)

    def active_x(k, slot):
        to = (x + k) % SIDE
        return remote(
            a_send.at[:, to], a_grid.at[y, slot], ax_ssem.at[k], ax_rsem.at[k], {"tp": y * SIDE + to}
        )

    def active_ref(p, k, part):
        block = a_grid.at[p, (x - k + SIDE) % SIDE]
        half = a_grid.shape[2] // 2
        return block if part is None else block.at[pl.ds(part * half, half)]

    ay = Ring(active_ref, lambda p: {"tp": p * SIDE + x}, ay_ssem, ay_rsem, y)
    groups = (1, 3, 2)
    for k in groups:
        active_x(k, x).start()
    a_grid[y, x] = a_send[:, x]
    ay.first(0)
    acc2[...] = jnp.zeros_like(acc2)
    share = acc2.shape[0]

    def multiply_down(step, k):
        p, g = (y + step + SIDE) % SIDE, (x - k + SIDE) % SIDE
        acc2[...] += lax.dot_general(
            a_grid[p, g].reshape(share, hid),
            d_grid[p, g],
            (((1,), (1,)), ((), ())),
            preferred_element_type=F32,
        )

    for k in (0,) + groups:
        dx.last(k)
    multiply_down(0, 0)
    for k in groups:
        active_x(k, (x - k + SIDE) % SIDE).wait_recv()
        ay.first(k)
    for k in groups:
        multiply_down(0, k)
    for k in (0,) + groups:
        ay.second(k)
        multiply_down(-1, k)
        multiply_down(1, k)
    for k in (0,) + groups:
        ay.last(k)
        multiply_down(2, k)

    for p in range(SIDE):
        part = acc2[:, p * fcols : (p + 1) * fcols].astype(BF)
        r_send[p] = part.reshape(r_send.shape[1:])

    def return_copy(q, core, p):
        chip = q * SIDE + x
        to = chip * 2 + core
        return remote(
            r_send.at[p, q * 2 + core],
            r_recv.at[f],
            r_ssem.at[(q * 2 + core) * SIDE + p],
            r_rsem.at[f],
            {"fs": to, "tp": y * SIDE + p},
        ), jnp.logical_and(to == f, p == x)

    def each_return(act):
        @pl.loop(0, n_z // SIDE)
        def _(k):
            q = (z // SIDE + n_z // SIDE // 2 + k) % (n_z // SIDE)
            for core in (0, 1):
                for p in range(SIDE):
                    c, local = return_copy(q, core, p)

                    @pl.when(jnp.logical_not(local))
                    def _():
                        act(c)

    each_return(lambda c: c.start())

    @pl.when(z % SIDE == x)
    def _():
        r_recv[f] = r_send[x, (z // SIDE) * 2 + c]

    drain_all(tokens_copy)
    drain_all(weights_copy)
    for k in groups:
        down_y(k, y).wait_send()
        active_x(k, x).wait_send()
    dx.drain()
    tg.drain()
    ay.drain()
    for store in stores:
        store.wait()

    @pl.loop(0, n_fs)
    def _(e):
        @pl.when(jnp.logical_not(jnp.logical_and(e == f, z % SIDE == x)))
        def _():
            remote(
                r_send.at[0, 0],
                r_recv.at[e],
                r_ssem.at[0],
                r_rsem.at[e],
                {"fs": e, "tp": y * SIDE + z % SIDE},
            ).wait_recv()

    back = r_recv[...].reshape(rows, fcols)
    mix = jnp.dot(high_v[...], back, preferred_element_type=F32) + jnp.dot(
        low_v[...], back, preferred_element_type=F32
    )
    mix_out[...] = mix.astype(BF)
    each_return(lambda c: c.wait_send())


def on_device(n_fs, n_tp, tokens, experts, routing, gain, gate_master, linear_master, down_weight):
    tok, top = experts.shape
    ecount, stripe, hid = gate_master.shape
    width = tokens.shape[1]
    fcols = width // n_tp
    cap = 3 * tok * top // (2 * ecount)
    tiles = ecount * cap // 8
    rows = ecount * cap
    vmem, any_space = pl.BlockSpec(memory_space=pltpu.VMEM), pl.BlockSpec(memory_space=pl.ANY)
    hbm = pl.BlockSpec(memory_space=pltpu.HBM)
    sources = ecount // SIDE
    dma = pltpu.SemaphoreType.DMA
    gate_out, linear_out, mix = pl.pallas_call(
        functools.partial(kernel, n_fs, n_tp),
        out_shape=(
            jax.ShapeDtypeStruct((ecount, stripe, hid), BF),
            jax.ShapeDtypeStruct((ecount, stripe, hid), BF),
            jax.ShapeDtypeStruct((tok, fcols), BF),
        ),
        in_specs=[hbm] * 7,
        out_specs=(any_space, any_space, vmem),
        scratch_shapes=[
            pltpu.VMEM((top, tok), jnp.int32),
            pltpu.VMEM((top, tok), F32),
            pltpu.VMEM((width // hid, hid), F32),
            pltpu.VMEM((ecount, stripe, hid), F32),
            pltpu.VMEM((ecount, stripe, hid), F32),
            pltpu.VMEM((tok, fcols), BF),
            pltpu.VMEM((SIDE, width // SIDE, hid), BF),
            pltpu.VMEM((ecount, stripe, 2 * hid), BF),
            pltpu.VMEM((ecount, stripe, 2 * hid), BF),
            pltpu.VMEM((tiles, 8, fcols), BF),
            pltpu.VMEM((n_tp, tiles, 8, fcols), BF),
            pltpu.VMEM((sources // 2, SIDE, cap // 4, 8, hid), BF),
            pltpu.VMEM((SIDE, SIDE, sources // 2, cap // 4, 8, hid), BF),
            pltpu.VMEM((SIDE, SIDE, width // SIDE, hid), BF),
            pltpu.VMEM((SIDE, sources, cap // 8, 8, fcols), BF),
            pltpu.VMEM((ecount, cap // 8, 8, fcols), BF),
            pltpu.VMEM((ecount, tok), F32),
            pltpu.VMEM((ecount, tok), F32),
            pltpu.VMEM((rows, tok), F32),
            pltpu.VMEM((rows, tok), F32),
            pltpu.VMEM((tok, rows), BF),
            pltpu.VMEM((tok, rows), BF),
            pltpu.VMEM((rows, 2 * hid), F32),
            pltpu.VMEM((rows // SIDE, width // SIDE), F32),
            dma((9,)),
            dma((n_fs,)),
            dma((n_fs,)),
            dma((n_fs,)),
            dma((n_fs,)),
            dma((n_fs,)),
            dma((n_fs,)),
            dma((SIDE,)),
            dma((SIDE,)),
            dma((16,)),
            dma((16,)),
            dma((40,)),
            dma((40,)),
            dma((SIDE,)),
            dma((SIDE,)),
            dma((16,)),
            dma((16,)),
        ],
        compiler_params=pltpu.CompilerParams(
            collective_id=0, has_side_effects=True, vmem_limit_bytes=67043328
        ),
    )(
        experts.T,
        routing.T,
        gain.reshape(width // hid, hid),
        tokens,
        gate_master,
        linear_master,
        down_weight.reshape(SIDE, width // SIDE, hid),
    )
    shape = (1, width, hid)
    return gate_out.reshape(shape), linear_out.reshape(shape), mix


def solution(mesh):
    n_fs, n_tp = mesh.shape["fs"], mesh.shape["tp"]
    return jax.shard_map(
        functools.partial(on_device, n_fs, n_tp),
        mesh=mesh,
        in_specs=(
            P("fs", None),
            P("fs", None),
            P("fs", None),
            P(),
            P(None, "fs", "tp"),
            P(None, "fs", "tp"),
            P("fs", None, "tp"),
        ),
        out_specs=(P("fs", None, "tp"), P("fs", None, "tp"), P("fs", "tp")),
        check_vma=False,
    )
```

```python
import functools

import jax
import jax.numpy as jnp
from jax import lax
from jax.experimental import pallas as pl
from jax.experimental.pallas import tpu as pltpu
from jax.sharding import PartitionSpec as P

clamp_limit = 7.0
gate_slope = 1.702
BF = jnp.bfloat16
F32 = jnp.float32
MESH = pl.DeviceIdType.MESH
SIDE = 4


def remote(src, dst, send_sem, recv_sem, device):
    return pltpu.make_async_remote_copy(
        src_ref=src,
        dst_ref=dst,
        send_sem=send_sem,
        recv_sem=recv_sem,
        device_id=device,
        device_id_type=MESH,
    )


class Torus:
    def __init__(self, grid, send_sems, recv_sems, t):
        self.grid, self.send_sems, self.recv_sems = grid, send_sems, recv_sems
        self.y, self.x = t // SIDE, t % SIDE
        tiles = grid.shape[1]
        self.half, self.quarter = tiles // 2, tiles // 4
        self.sent = []

    def at(self, h, a, b):
        dx, dy = (a, b) if h == 0 else (b, a)
        return ((self.y + dy + SIDE) % SIDE) * SIDE + (self.x + dx + SIDE) % SIDE

    def copy(self, h, slot, a, b, part, to):
        start = h * self.half + (self.quarter if part == 1 else 0)
        size = self.half if part is None else self.quarter
        ref = self.grid.at[self.at(h, a, b), pl.ds(start, size)]
        k = h * 20 + slot
        return remote(ref, ref, self.send_sems.at[k], self.recv_sems.at[k], {"tp": self.at(h, *to)})

    def send(self, h, slot, a, b, part, to):
        c = self.copy(h, slot, a, b, part, to)
        c.start()
        self.sent.append(c)

    def recv(self, h, slot, a, b, part):
        self.copy(h, slot, a, b, part, (1, 0)).wait_recv()

    def own(self):
        for h in (0, 1):
            self.send(h, 0, 0, 0, None, (1, 0))
            self.send(h, 1, 0, 0, None, (-1, 0))
            self.column(h, 0, 0)

    def column(self, h, i, a):
        self.send(h, 4 + 4 * i, a, 0, None, (0, 1))
        self.send(h, 5 + 4 * i, a, 0, None, (0, -1))

    def turn(self, h, i, a):
        self.recv(h, 4 + 4 * i, a, -1, None)
        self.send(h, 6 + 4 * i, a, -1, 0, (0, 1))
        self.recv(h, 5 + 4 * i, a, 1, None)
        self.send(h, 7 + 4 * i, a, 1, 1, (0, -1))

    def rest(self):
        for h in (0, 1):
            self.recv(h, 0, -1, 0, None)
            self.send(h, 2, -1, 0, 0, (1, 0))
            self.column(h, 1, -1)
            self.recv(h, 1, 1, 0, None)
            self.send(h, 3, 1, 0, 1, (-1, 0))
            self.column(h, 2, 1)
        for h in (0, 1):
            self.turn(h, 0, 0)
        for h in (0, 1):
            self.recv(h, 2, 2, 0, 0)
            self.recv(h, 3, 2, 0, 1)
            self.column(h, 3, 2)
        for h in (0, 1):
            self.turn(h, 1, -1)
            self.turn(h, 2, 1)
        for h in (0, 1):
            self.turn(h, 3, 2)
        for h in (0, 1):
            for i, a in enumerate((0, -1, 1, 2)):
                self.recv(h, 6 + 4 * i, a, 2, 0)
                self.recv(h, 7 + 4 * i, a, 2, 1)

    def drain(self):
        for c in self.sent:
            c.wait_send()


class Ring:
    def __init__(self, ref_of, device_of, send_sems, recv_sems, pos):
        self.ref_of, self.device_of, self.pos = ref_of, device_of, pos
        self.send_sems, self.recv_sems, self.sent = send_sems, recv_sems, []

    def at(self, step):
        return (self.pos + step + SIDE) % SIDE

    def copy(self, item, slot, step, part, to):
        ref = self.ref_of(self.at(step), item, part)
        k = item * 4 + slot
        return remote(
            ref, ref, self.send_sems.at[k], self.recv_sems.at[k], self.device_of(self.at(to))
        )

    def send(self, item, slot, step, part, to):
        c = self.copy(item, slot, step, part, to)
        c.start()
        self.sent.append(c)

    def first(self, item):
        self.send(item, 0, 0, None, 1)
        self.send(item, 1, 0, None, -1)

    def second(self, item):
        self.copy(item, 0, -1, None, 1).wait_recv()
        self.send(item, 2, -1, 0, 1)
        self.copy(item, 1, 1, None, 1).wait_recv()
        self.send(item, 3, 1, 1, -1)

    def last(self, item):
        self.copy(item, 2, 2, 0, 1).wait_recv()
        self.copy(item, 3, 2, 1, 1).wait_recv()

    def drain(self):
        for c in self.sent:
            c.wait_send()


def kernel(
    n_fs,
    n_tp,
    experts_hbm,
    routing_hbm,
    gain_hbm,
    tokens_hbm,
    gate_hbm,
    linear_hbm,
    down_hbm,
    gate_out,
    linear_out,
    mix_out,
    experts_ref,
    routing_ref,
    gain_ref,
    gate_v,
    linear_v,
    tok_v,
    down_v,
    w_send,
    w_recv,
    t_send,
    t_grid,
    a_send,
    a_grid,
    d_grid,
    r_send,
    r_recv,
    slot_v,
    weight_v,
    pick_v,
    mixer_v,
    high_v,
    low_v,
    acc,
    acc2,
    local_sems,
    t_ssem,
    t_rsem,
    w_ssem,
    w_rsem,
    r_ssem,
    r_rsem,
    dy_ssem,
    dy_rsem,
    dx_ssem,
    dx_rsem,
    tg_ssem,
    tg_rsem,
    ax_ssem,
    ax_rsem,
    ay_ssem,
    ay_rsem,
):
    f, t = lax.axis_index("fs"), lax.axis_index("tp")
    n_z = n_fs // 2
    z, c = f // 2, f % 2
    stripe, hid = gate_v.shape[1], gate_v.shape[2]
    fcols = tok_v.shape[1]
    tok = tok_v.shape[0]
    tiles = t_grid.shape[1]
    rows = tiles * 8
    per = tiles // n_fs
    cap = per * 8

    y, x = t // SIDE, t % SIDE
    loads = [
        pltpu.make_async_copy(
            tokens_hbm.at[:, pl.ds(pl.multiple_of(t * fcols, 128), fcols)], tok_v, local_sems.at[0]
        ),
        pltpu.make_async_copy(gate_hbm, gate_v, local_sems.at[1]),
        pltpu.make_async_copy(linear_hbm, linear_v, local_sems.at[2]),
        pltpu.make_async_copy(down_hbm, down_v, local_sems.at[3]),
        pltpu.make_async_copy(experts_hbm, experts_ref, local_sems.at[4]),
        pltpu.make_async_copy(routing_hbm, routing_ref, local_sems.at[5]),
        pltpu.make_async_copy(gain_hbm, gain_ref, local_sems.at[6]),
    ]
    for load in loads:
        load.start()

    barrier = pltpu.get_barrier_semaphore()

    @pl.loop(1, n_fs)
    def _(k):
        pl.semaphore_signal(
            barrier, inc=1, device_id={"fs": (f + k) % n_fs}, device_id_type=MESH
        )

    @pl.loop(1, n_tp)
    def _(k):
        pl.semaphore_signal(
            barrier, inc=1, device_id={"tp": (t + k) % n_tp}, device_id_type=MESH
        )

    loads[4].wait()
    loads[5].wait()
    names = lax.broadcasted_iota(jnp.int32, (n_fs, tok), 0)
    chosen = jnp.zeros((n_fs, tok), F32)
    weight = jnp.zeros((n_fs, tok), F32)
    for k in range(experts_ref.shape[0]):
        hit = experts_ref[k : k + 1, :] == names
        chosen = chosen + jnp.where(hit, 1.0, 0.0)
        weight = weight + jnp.where(hit, routing_ref[k : k + 1, :], 0.0)
    before = jnp.where(
        lax.broadcasted_iota(jnp.int32, (tok, tok), 0)
        < lax.broadcasted_iota(jnp.int32, (tok, tok), 1),
        1.0,
        0.0,
    ).astype(BF)
    rank = jnp.dot(chosen.astype(BF), before, preferred_element_type=F32)
    slot_v[...] = jnp.where(chosen > 0.0, rank, -1.0)
    weight_v[...] = weight
    places = lax.broadcasted_iota(jnp.int32, (cap, tok), 0).astype(F32)

    @pl.loop(0, n_fs)
    def _(e):
        hit = slot_v[pl.ds(e, 1), :] == places
        at = pl.ds(pl.multiple_of(e * cap, 8), cap)
        pick_v[at, :] = jnp.where(hit, 1.0, 0.0)
        mixer_v[at, :] = jnp.where(hit, weight_v[pl.ds(e, 1), :], 0.0)

    loads[0].wait()
    sent = jnp.dot(pick_v[...].astype(BF), tok_v[...], preferred_element_type=F32)
    t_send[...] = sent.astype(BF).reshape(tiles, 8, fcols)

    loads[6].wait()
    here = lax.broadcasted_iota(jnp.int32, (stripe, hid), 0) + (f * stripe) % hid
    lane = lax.broadcasted_iota(jnp.int32, (stripe, hid), 1)
    picked = jnp.where(here == lane, gain_ref[pl.ds((f * stripe) // hid, 1), :], 0.0)
    column = jnp.sum(picked, axis=1, keepdims=True)
    loads[1].wait()
    loads[2].wait()

    @pl.loop(0, n_fs)
    def _(e):
        w_send[e, :, 0:hid] = (gate_v[e] * column).astype(BF)
        w_send[e, :, hid : 2 * hid] = (linear_v[e] * column).astype(BF)

    loads[3].wait()
    pl.semaphore_wait(barrier, n_fs + n_tp - 2)

    def tile_span(i):
        return pl.ds(i * per, per)

    def peer(dz, dc):
        return ((z + dz) % n_z) * 2 + (c + dc) % 2

    def source(dz, dc):
        return ((z - dz + n_z) % n_z) * 2 + (c + dc) % 2

    def turn(k):
        return (n_z // 2 + (1 - 2 * (k % 2)) * ((k + 1) // 2)) % n_z

    def tokens_copy(dz, dc, to, slot):
        i = dz * 2 + dc
        return remote(
            t_send.at[tile_span(to)],
            t_grid.at[t, tile_span(slot)],
            t_ssem.at[i],
            t_rsem.at[i],
            {"fs": to},
        )

    def weights_copy(dz, dc, to, slot):
        i = dz * 2 + dc
        return remote(w_send.at[to], w_recv.at[slot], w_ssem.at[i], w_rsem.at[i], {"fs": to})

    def start_all(copy):
        @pl.loop(0, n_z - 1)
        def _(k):
            dz = turn(k)
            for dc in (0, 1):
                copy(dz, dc, peer(dz, dc), f).start()

        copy(0, 1, peer(0, 1), f).start()

    def recv_all(copy):
        copy(0, 1, peer(0, 1), source(0, 1)).wait_recv()

        @pl.loop(0, n_z - 1)
        def _(k):
            dz = turn(k)
            for dc in (0, 1):
                copy(dz, dc, peer(dz, dc), source(dz, dc)).wait_recv()

    def drain_all(copy):
        copy(0, 1, peer(0, 1), f).wait_send()

        @pl.loop(0, n_z - 1)
        def _(k):
            dz = turn(k)
            for dc in (0, 1):
                copy(dz, dc, peer(dz, dc), f).wait_send()

    def down_y(k, slot):
        to = (y + k) % SIDE
        return remote(
            down_v.at[to], d_grid.at[slot, x], dy_ssem.at[k], dy_rsem.at[k], {"tp": to * SIDE + x}
        )

    def down_ref(p, k, part):
        block = d_grid.at[(y - k + SIDE) % SIDE, p]
        half = d_grid.shape[2] // 2
        return block if part is None else block.at[pl.ds(part * half, half)]

    dx = Ring(down_ref, lambda p: {"tp": y * SIDE + p}, dx_ssem, dx_rsem, x)

    start_all(tokens_copy)
    start_all(weights_copy)

    for k in (1, 3, 2):
        down_y(k, y).start()
    d_grid[y, x] = down_v[y]
    dx.first(0)

    t_grid[t, tile_span(f)] = t_send[tile_span(f)]
    w_recv[f] = w_send[f]
    for j in range(rows // 128):
        at = slice(j * 128, (j + 1) * 128)
        turned = mixer_v[at, :].T
        high = turned.astype(BF)
        high_v[:, at] = high
        low_v[:, at] = (turned - high.astype(F32)).astype(BF)
    acc[...] = jnp.zeros_like(acc)

    for k in (1, 3, 2):
        down_y(k, (y - k + SIDE) % SIDE).wait_recv()
        dx.first(k)

    recv_all(tokens_copy)
    tg = Torus(t_grid, tg_ssem, tg_rsem, t)
    tg.own()
    for k in (0, 1, 3, 2):
        dx.second(k)
    tg.rest()

    def lhs(chip):
        return t_grid[chip].reshape(rows, fcols)

    def rhs(chip):
        return w_recv[pl.ds(chip * 2, 2)].reshape(fcols, 2 * hid)

    def multiply(one, other):
        acc[...] += jnp.dot(
            jnp.concatenate([lhs(one), lhs(other)], axis=1),
            jnp.concatenate([rhs(one), rhs(other)], axis=0),
            preferred_element_type=F32,
        )

    def weights_of(dz):
        for dc in (0, 1):
            weights_copy(dz, dc, peer(dz, dc), source(dz, dc)).wait_recv()
        return (z - dz + n_z) % n_z

    weights_copy(0, 1, peer(0, 1), source(0, 1)).wait_recv()
    multiply(z, weights_of(n_z // 2))

    @pl.loop(1, n_z // 2)
    def _(k):
        multiply(weights_of(n_z // 2 - k), weights_of(n_z // 2 + k))

    stores = [
        pltpu.make_async_copy(w_recv.at[:, :, pl.ds(0, hid)], gate_out, local_sems.at[7]),
        pltpu.make_async_copy(w_recv.at[:, :, pl.ds(hid, hid)], linear_out, local_sems.at[8]),
    ]
    for store in stores:
        store.start()

    n_q = a_send.shape[0]
    offsets = (4, 5, 3, 0, 6, 2, 7, 1)
    chunk = n_q // 2
    span = rows // n_q
    groups = (1, 3, 2)

    def q_of(j):
        return (z // 2 + offsets[j]) % n_q

    def active_x(r, k, slot):
        to = (x + k) % SIDE
        i = r * SIDE + k
        return remote(
            a_send.at[pl.ds(r * chunk, chunk), to],
            a_grid.at[y, slot, pl.ds(r * chunk, chunk)],
            ax_ssem.at[i],
            ax_rsem.at[i],
            {"tp": y * SIDE + to},
        )

    def active_ref(p, item, part):
        r, k = item // SIDE, item % SIDE
        block = a_grid.at[p, (x - k + SIDE) % SIDE]
        half = chunk // 2
        if part is None:
            return block.at[pl.ds(r * chunk, chunk)]
        return block.at[pl.ds(r * chunk + part * half, half)]

    ay = Ring(active_ref, lambda p: {"tp": p * SIDE + x}, ay_ssem, ay_rsem, y)

    for r in (0, 1):
        for j in range(r * chunk, (r + 1) * chunk):
            at = pl.ds(pl.multiple_of(q_of(j) * span, 8), span)
            clamped = jnp.minimum(acc[at, 0:hid], clamp_limit)
            linear = jnp.clip(acc[at, hid : 2 * hid], -clamp_limit, clamp_limit)
            active = clamped * jax.nn.sigmoid(gate_slope * clamped) * (linear + 1.0)
            a_send[j] = active.astype(BF).reshape(a_send.shape[1:])
        for k in groups:
            active_x(r, k, x).start()
        at = pl.ds(r * chunk, chunk)
        a_grid[y, x, at] = a_send[at, x]
        if r == 0:
            ay.first(0)

    acc2[...] = jnp.zeros_like(acc2)
    share = acc2.shape[1]

    def multiply_down(r, step, k, k2):
        p = (y + step + SIDE) % SIDE
        g, g2 = (x - k + SIDE) % SIDE, (x - k2 + SIDE) % SIDE
        at = pl.ds(r * chunk, chunk)
        acc2[r] += lax.dot_general(
            jnp.concatenate(
                [a_grid[p, g, at].reshape(share, hid), a_grid[p, g2, at].reshape(share, hid)], axis=1
            ),
            jnp.concatenate([d_grid[p, g], d_grid[p, g2]], axis=1),
            (((1,), (1,)), ((), ())),
            preferred_element_type=F32,
        )

    def return_copy(j, p):
        to = q_of(j) * SIDE + x
        return remote(
            r_send.at[p, j],
            r_recv.at[f],
            r_ssem.at[j * SIDE + p],
            r_rsem.at[f],
            {"fs": to, "tp": y * SIDE + p},
        ), jnp.logical_and(to == f, p == x)

    def each_return(r, act):
        for j in range(r * chunk, (r + 1) * chunk):
            for p in range(SIDE):
                c, local = return_copy(j, p)
                if offsets[j] != 0:
                    act(c)
                else:

                    @pl.when(jnp.logical_not(local))
                    def _():
                        act(c)

    def give_back(r):
        for p in range(SIDE):
            part = acc2[r, :, p * fcols : (p + 1) * fcols].astype(BF)
            r_send[p, pl.ds(r * chunk, chunk)] = part.reshape(chunk, *r_send.shape[2:])
        each_return(r, lambda c: c.start())

    for k in groups:
        active_x(0, k, (x - k + SIDE) % SIDE).wait_recv()
        ay.first(k)
    for k in (0,) + groups:
        dx.last(k)
    multiply_down(0, 0, 0, 1)
    multiply_down(0, 0, 3, 2)
    for k in (0,) + groups:
        ay.second(k)
        if k > 0:
            active_x(1, k, (x - k + SIDE) % SIDE).wait_recv()
        ay.first(SIDE + k)
    for step in (-1, 1):
        multiply_down(0, step, 0, 1)
        multiply_down(0, step, 3, 2)
    for k in (0,) + groups:
        ay.second(SIDE + k)
    for k in (0,) + groups:
        ay.last(k)
    multiply_down(0, 2, 0, 1)
    multiply_down(0, 2, 3, 2)
    give_back(0)
    for step in (0, -1, 1):
        multiply_down(1, step, 0, 1)
        multiply_down(1, step, 3, 2)
    for k in (0,) + groups:
        ay.last(SIDE + k)
    multiply_down(1, 2, 0, 1)
    multiply_down(1, 2, 3, 2)
    give_back(1)

    @pl.when(f % SIDE == x)
    def _():
        r_recv[f] = r_send[x, offsets.index(0)]

    drain_all(tokens_copy)
    drain_all(weights_copy)
    for k in groups:
        down_y(k, y).wait_send()
        active_x(0, k, x).wait_send()
        active_x(1, k, x).wait_send()
    dx.drain()
    tg.drain()
    ay.drain()
    for store in stores:
        store.wait()

    @pl.loop(0, n_fs)
    def _(e):
        @pl.when(jnp.logical_not(jnp.logical_and(e == f, f % SIDE == x)))
        def _():
            remote(
                r_send.at[0, 0],
                r_recv.at[e],
                r_ssem.at[0],
                r_rsem.at[e],
                {"fs": e, "tp": y * SIDE + f % SIDE},
            ).wait_recv()

    back = r_recv[...].reshape(rows, fcols)
    mix = jnp.dot(high_v[...], back, preferred_element_type=F32) + jnp.dot(
        low_v[...], back, preferred_element_type=F32
    )
    mix_out[...] = mix.astype(BF)
    each_return(0, lambda c: c.wait_send())
    each_return(1, lambda c: c.wait_send())


def copy_out(a, b, c, a_out, b_out, c_out, sems):
    copies = [
        pltpu.make_async_copy(src, dst, sems.at[i])
        for i, (src, dst) in enumerate(((a, a_out), (b, b_out), (c, c_out)))
    ]
    for copy in copies:
        copy.start()
    for copy in copies:
        copy.wait()


def on_device(n_fs, n_tp, tokens, experts, routing, gain, gate_master, linear_master, down_weight):
    tok, top = experts.shape
    ecount, stripe, hid = gate_master.shape
    width = tokens.shape[1]
    fcols = width // n_tp
    cap = 3 * tok * top // (2 * ecount)
    tiles = ecount * cap // 8
    rows = ecount * cap
    vmem, any_space = pl.BlockSpec(memory_space=pltpu.VMEM), pl.BlockSpec(memory_space=pl.ANY)
    hbm = pl.BlockSpec(memory_space=pltpu.HBM)
    sources = ecount // SIDE
    dma = pltpu.SemaphoreType.DMA
    gate_out, linear_out, mix = pl.pallas_call(
        functools.partial(kernel, n_fs, n_tp),
        out_shape=(
            jax.ShapeDtypeStruct((ecount, stripe, hid), BF),
            jax.ShapeDtypeStruct((ecount, stripe, hid), BF),
            jax.ShapeDtypeStruct((tok, fcols), BF),
        ),
        in_specs=[hbm] * 7,
        out_specs=(any_space, any_space, vmem),
        scratch_shapes=[
            pltpu.VMEM((top, tok), jnp.int32),
            pltpu.VMEM((top, tok), F32),
            pltpu.VMEM((width // hid, hid), F32),
            pltpu.VMEM((ecount, stripe, hid), F32),
            pltpu.VMEM((ecount, stripe, hid), F32),
            pltpu.VMEM((tok, fcols), BF),
            pltpu.VMEM((SIDE, width // SIDE, hid), BF),
            pltpu.VMEM((ecount, stripe, 2 * hid), BF),
            pltpu.VMEM((ecount, stripe, 2 * hid), BF),
            pltpu.VMEM((tiles, 8, fcols), BF),
            pltpu.VMEM((n_tp, tiles, 8, fcols), BF),
            pltpu.VMEM((sources, SIDE, cap // 8, 8, hid), BF),
            pltpu.VMEM((SIDE, SIDE, sources, cap // 8, 8, hid), BF),
            pltpu.VMEM((SIDE, SIDE, width // SIDE, hid), BF),
            pltpu.VMEM((SIDE, sources, cap // 8, 8, fcols), BF),
            pltpu.VMEM((ecount, cap // 8, 8, fcols), BF),
            pltpu.VMEM((ecount, tok), F32),
            pltpu.VMEM((ecount, tok), F32),
            pltpu.VMEM((rows, tok), F32),
            pltpu.VMEM((rows, tok), F32),
            pltpu.VMEM((tok, rows), BF),
            pltpu.VMEM((tok, rows), BF),
            pltpu.VMEM((rows, 2 * hid), F32),
            pltpu.VMEM((2, rows // SIDE // 2, width // SIDE), F32),
            dma((9,)),
            dma((n_fs,)),
            dma((n_fs,)),
            dma((n_fs,)),
            dma((n_fs,)),
            dma((n_fs,)),
            dma((n_fs,)),
            dma((SIDE,)),
            dma((SIDE,)),
            dma((16,)),
            dma((16,)),
            dma((40,)),
            dma((40,)),
            dma((2 * SIDE,)),
            dma((2 * SIDE,)),
            dma((32,)),
            dma((32,)),
        ],
        compiler_params=pltpu.CompilerParams(
            collective_id=0, has_side_effects=True, vmem_limit_bytes=48 * 1024 * 1024
        ),
    )(
        *[
            pltpu.with_memory_space_constraint(v, pltpu.HBM)
            for v in (
                experts.T,
                routing.T,
                gain.reshape(width // hid, hid),
                tokens,
                gate_master,
                linear_master,
                down_weight.reshape(SIDE, width // SIDE, hid),
            )
        ]
    )
    shape = (1, width, hid)
    results = (gate_out.reshape(shape), linear_out.reshape(shape), mix)
    return pl.pallas_call(
        copy_out,
        out_shape=tuple(jax.ShapeDtypeStruct(v.shape, v.dtype) for v in results),
        in_specs=[vmem] * 3,
        out_specs=(hbm,) * 3,
        scratch_shapes=[dma((3,))],
    )(*[pltpu.with_memory_space_constraint(v, pltpu.VMEM) for v in results])


def solution(mesh):
    n_fs, n_tp = mesh.shape["fs"], mesh.shape["tp"]
    return jax.shard_map(
        functools.partial(on_device, n_fs, n_tp),
        mesh=mesh,
        in_specs=(
            P("fs", None),
            P("fs", None),
            P("fs", None),
            P(),
            P(None, "fs", "tp"),
            P(None, "fs", "tp"),
            P("fs", None, "tp"),
        ),
        out_specs=(P("fs", None, "tp"), P("fs", None, "tp"), P("fs", "tp")),
        check_vma=False,
    )
```

```python
import functools

import jax
import jax.numpy as jnp
from jax import lax
from jax.experimental import pallas as pl
from jax.experimental.pallas import tpu as pltpu
from jax.sharding import PartitionSpec as P

clamp_limit = 7.0
gate_slope = 1.702
BF = jnp.bfloat16
F32 = jnp.float32
MESH = pl.DeviceIdType.MESH
CHUNKS = 4
SIDE = 4


def remote(src, dst, send_sem, recv_sem, device):
    return pltpu.make_async_remote_copy(
        src_ref=src,
        dst_ref=dst,
        send_sem=send_sem,
        recv_sem=recv_sem,
        device_id=device,
        device_id_type=MESH,
    )


class Torus:
    def __init__(self, grid, send_sems, recv_sems, t):
        self.grid, self.send_sems, self.recv_sems = grid, send_sems, recv_sems
        self.y, self.x = t // SIDE, t % SIDE
        tiles = grid.shape[1]
        self.half, self.quarter = tiles // 2, tiles // 4
        self.sent = []

    def at(self, h, a, b):
        dx, dy = (a, b) if h == 0 else (b, a)
        return ((self.y + dy + SIDE) % SIDE) * SIDE + (self.x + dx + SIDE) % SIDE

    def copy(self, h, slot, a, b, part, to):
        start = h * self.half + (self.quarter if part == 1 else 0)
        size = self.half if part is None else self.quarter
        ref = self.grid.at[self.at(h, a, b), pl.ds(start, size)]
        k = h * 20 + slot
        return remote(ref, ref, self.send_sems.at[k], self.recv_sems.at[k], {"tp": self.at(h, *to)})

    def send(self, h, slot, a, b, part, to):
        c = self.copy(h, slot, a, b, part, to)
        c.start()
        self.sent.append(c)

    def recv(self, h, slot, a, b, part):
        self.copy(h, slot, a, b, part, (1, 0)).wait_recv()

    def own(self):
        for h in (0, 1):
            self.send(h, 0, 0, 0, None, (1, 0))
            self.send(h, 1, 0, 0, None, (-1, 0))
            self.column(h, 0, 0)

    def column(self, h, i, a):
        self.send(h, 4 + 4 * i, a, 0, None, (0, 1))
        self.send(h, 5 + 4 * i, a, 0, None, (0, -1))

    def turn(self, h, i, a):
        self.recv(h, 4 + 4 * i, a, -1, None)
        self.send(h, 6 + 4 * i, a, -1, 0, (0, 1))
        self.recv(h, 5 + 4 * i, a, 1, None)
        self.send(h, 7 + 4 * i, a, 1, 1, (0, -1))

    def rest(self):
        for h in (0, 1):
            self.recv(h, 0, -1, 0, None)
            self.send(h, 2, -1, 0, 0, (1, 0))
            self.column(h, 1, -1)
            self.recv(h, 1, 1, 0, None)
            self.send(h, 3, 1, 0, 1, (-1, 0))
            self.column(h, 2, 1)
        for h in (0, 1):
            self.turn(h, 0, 0)
        for h in (0, 1):
            self.recv(h, 2, 2, 0, 0)
            self.recv(h, 3, 2, 0, 1)
            self.column(h, 3, 2)
        for h in (0, 1):
            self.turn(h, 1, -1)
            self.turn(h, 2, 1)
        for h in (0, 1):
            self.turn(h, 3, 2)
        for h in (0, 1):
            for i, a in enumerate((0, -1, 1, 2)):
                self.recv(h, 6 + 4 * i, a, 2, 0)
                self.recv(h, 7 + 4 * i, a, 2, 1)

    def drain(self):
        for c in self.sent:
            c.wait_send()


class Ring:
    def __init__(self, ref_of, device_of, send_sems, recv_sems, pos):
        self.ref_of, self.device_of, self.pos = ref_of, device_of, pos
        self.send_sems, self.recv_sems, self.sent = send_sems, recv_sems, []

    def at(self, step):
        return (self.pos + step + SIDE) % SIDE

    def copy(self, item, slot, step, part, to):
        ref = self.ref_of(self.at(step), item, part)
        k = item * 4 + slot
        return remote(
            ref, ref, self.send_sems.at[k], self.recv_sems.at[k], self.device_of(self.at(to))
        )

    def send(self, item, slot, step, part, to):
        c = self.copy(item, slot, step, part, to)
        c.start()
        self.sent.append(c)

    def first(self, item):
        self.send(item, 0, 0, None, 1)
        self.send(item, 1, 0, None, -1)

    def second(self, item):
        self.copy(item, 0, -1, None, 1).wait_recv()
        self.send(item, 2, -1, 0, 1)
        self.copy(item, 1, 1, None, 1).wait_recv()
        self.send(item, 3, 1, 1, -1)

    def last(self, item):
        self.copy(item, 2, 2, 0, 1).wait_recv()
        self.copy(item, 3, 2, 1, 1).wait_recv()

    def drain(self):
        for c in self.sent:
            c.wait_send()


def kernel(
    n_fs,
    n_tp,
    experts_hbm,
    routing_hbm,
    gain_hbm,
    tokens_hbm,
    gate_hbm,
    linear_hbm,
    down_hbm,
    gate_out,
    linear_out,
    mix_out,
    experts_ref,
    routing_ref,
    gain_ref,
    gate_v,
    linear_v,
    tok_v,
    down_v,
    w_send,
    w_recv,
    t_send,
    t_grid,
    a_send,
    a_grid,
    d_grid,
    r_send,
    r_recv,
    slot_v,
    weight_v,
    pick_v,
    mixer_v,
    high_v,
    low_v,
    acc,
    local_sems,
    t_ssem,
    t_rsem,
    w_ssem,
    w_rsem,
    r_ssem,
    r_rsem,
    dy_ssem,
    dy_rsem,
    dx_ssem,
    dx_rsem,
    tg_ssem,
    tg_rsem,
    a_ssem,
    a_rsem,
):
    f, t = lax.axis_index("fs"), lax.axis_index("tp")
    n_z = n_fs // 2
    z, c = f // 2, f % 2
    stripe, hid = gate_v.shape[1], gate_v.shape[2]
    fcols = tok_v.shape[1]
    tok = tok_v.shape[0]
    tiles = t_grid.shape[1]
    rows = tiles * 8
    per = tiles // n_fs
    cap = per * 8

    y, x = t // SIDE, t % SIDE
    loads = [
        pltpu.make_async_copy(
            tokens_hbm.at[:, pl.ds(pl.multiple_of(t * fcols, 128), fcols)], tok_v, local_sems.at[0]
        ),
        pltpu.make_async_copy(gate_hbm, gate_v, local_sems.at[1]),
        pltpu.make_async_copy(linear_hbm, linear_v, local_sems.at[2]),
        pltpu.make_async_copy(down_hbm, down_v, local_sems.at[3]),
        pltpu.make_async_copy(experts_hbm, experts_ref, local_sems.at[4]),
        pltpu.make_async_copy(routing_hbm, routing_ref, local_sems.at[5]),
        pltpu.make_async_copy(gain_hbm, gain_ref, local_sems.at[6]),
    ]
    for load in loads:
        load.start()

    barrier = pltpu.get_barrier_semaphore()

    @pl.loop(1, n_fs)
    def _(k):
        pl.semaphore_signal(
            barrier, inc=1, device_id={"fs": (f + k) % n_fs}, device_id_type=MESH
        )

    @pl.loop(1, n_tp)
    def _(k):
        pl.semaphore_signal(
            barrier, inc=1, device_id={"tp": (t + k) % n_tp}, device_id_type=MESH
        )

    loads[4].wait()
    loads[5].wait()
    names = lax.broadcasted_iota(jnp.int32, (n_fs, tok), 0)
    chosen = jnp.zeros((n_fs, tok), F32)
    weight = jnp.zeros((n_fs, tok), F32)
    for k in range(experts_ref.shape[0]):
        hit = experts_ref[k : k + 1, :] == names
        chosen = chosen + jnp.where(hit, 1.0, 0.0)
        weight = weight + jnp.where(hit, routing_ref[k : k + 1, :], 0.0)
    before = jnp.where(
        lax.broadcasted_iota(jnp.int32, (tok, tok), 0)
        < lax.broadcasted_iota(jnp.int32, (tok, tok), 1),
        1.0,
        0.0,
    ).astype(BF)
    rank = jnp.dot(chosen.astype(BF), before, preferred_element_type=F32)
    slot_v[...] = jnp.where(chosen > 0.0, rank, -1.0)
    weight_v[...] = weight
    places = lax.broadcasted_iota(jnp.int32, (cap, tok), 0).astype(F32)

    @pl.loop(0, n_fs)
    def _(e):
        hit = slot_v[pl.ds(e, 1), :] == places
        at = pl.ds(pl.multiple_of(e * cap, 8), cap)
        pick_v[at, :] = jnp.where(hit, 1.0, 0.0)
        mixer_v[at, :] = jnp.where(hit, weight_v[pl.ds(e, 1), :], 0.0)

    loads[0].wait()
    sent = jnp.dot(pick_v[...].astype(BF), tok_v[...], preferred_element_type=F32)
    t_send[...] = sent.astype(BF).reshape(tiles, 8, fcols)

    loads[6].wait()
    here = lax.broadcasted_iota(jnp.int32, (stripe, hid), 0) + (f * stripe) % hid
    lane = lax.broadcasted_iota(jnp.int32, (stripe, hid), 1)
    picked = jnp.where(here == lane, gain_ref[pl.ds((f * stripe) // hid, 1), :], 0.0)
    column = jnp.sum(picked, axis=1, keepdims=True)
    loads[1].wait()
    loads[2].wait()

    @pl.loop(0, n_fs)
    def _(e):
        w_send[e, :, 0:hid] = (gate_v[e] * column).astype(BF)
        w_send[e, :, hid : 2 * hid] = (linear_v[e] * column).astype(BF)

    loads[3].wait()
    pl.semaphore_wait(barrier, n_fs + n_tp - 2)

    def tile_span(i):
        return pl.ds(i * per, per)

    def peer(dz, dc):
        return ((z + dz) % n_z) * 2 + (c + dc) % 2

    def source(dz, dc):
        return ((z - dz + n_z) % n_z) * 2 + (c + dc) % 2

    def turn(k):
        return (n_z // 2 + (1 - 2 * (k % 2)) * ((k + 1) // 2)) % n_z

    def tokens_copy(dz, dc, to, slot):
        i = dz * 2 + dc
        return remote(
            t_send.at[tile_span(to)],
            t_grid.at[t, tile_span(slot)],
            t_ssem.at[i],
            t_rsem.at[i],
            {"fs": to},
        )

    def weights_copy(dz, dc, to, slot):
        i = dz * 2 + dc
        return remote(w_send.at[to], w_recv.at[slot], w_ssem.at[i], w_rsem.at[i], {"fs": to})

    def start_all(copy):
        @pl.loop(0, n_z - 1)
        def _(k):
            dz = turn(k)
            for dc in (0, 1):
                copy(dz, dc, peer(dz, dc), f).start()

        copy(0, 1, peer(0, 1), f).start()

    def recv_all(copy):
        copy(0, 1, peer(0, 1), source(0, 1)).wait_recv()

        @pl.loop(0, n_z - 1)
        def _(k):
            dz = turn(k)
            for dc in (0, 1):
                copy(dz, dc, peer(dz, dc), source(dz, dc)).wait_recv()

    def drain_all(copy):
        copy(0, 1, peer(0, 1), f).wait_send()

        @pl.loop(0, n_z - 1)
        def _(k):
            dz = turn(k)
            for dc in (0, 1):
                copy(dz, dc, peer(dz, dc), f).wait_send()

    def down_y(k, slot):
        to = (y + k) % SIDE
        return remote(
            down_v.at[to], d_grid.at[slot, x], dy_ssem.at[k], dy_rsem.at[k], {"tp": to * SIDE + x}
        )

    def down_ref(p, k, part):
        block = d_grid.at[(y - k + SIDE) % SIDE, p]
        half = d_grid.shape[2] // 2
        return block if part is None else block.at[pl.ds(part * half, half)]

    dx = Ring(down_ref, lambda p: {"tp": y * SIDE + p}, dx_ssem, dx_rsem, x)

    start_all(tokens_copy)
    start_all(weights_copy)

    for k in (1, 3, 2):
        down_y(k, y).start()
    d_grid[y, x] = down_v[y]
    dx.first(0)

    t_grid[t, tile_span(f)] = t_send[tile_span(f)]
    w_recv[f] = w_send[f]
    for j in range(rows // 128):
        at = slice(j * 128, (j + 1) * 128)
        turned = mixer_v[at, :].T
        high = turned.astype(BF)
        high_v[:, at] = high
        low_v[:, at] = (turned - high.astype(F32)).astype(BF)
    acc[...] = jnp.zeros_like(acc)

    for k in (1, 3, 2):
        down_y(k, (y - k + SIDE) % SIDE).wait_recv()
        dx.first(k)

    recv_all(tokens_copy)
    tg = Torus(t_grid, tg_ssem, tg_rsem, t)
    tg.own()
    for k in (0, 1, 3, 2):
        dx.second(k)
    tg.rest()

    def lhs(chip):
        return t_grid[chip].reshape(rows, fcols)

    def rhs(chip):
        return w_recv[pl.ds(chip * 2, 2)].reshape(fcols, 2 * hid)

    def multiply(one, other):
        acc[...] += jnp.dot(
            jnp.concatenate([lhs(one), lhs(other)], axis=1),
            jnp.concatenate([rhs(one), rhs(other)], axis=0),
            preferred_element_type=F32,
        )

    def weights_of(dz):
        for dc in (0, 1):
            weights_copy(dz, dc, peer(dz, dc), source(dz, dc)).wait_recv()
        return (z - dz + n_z) % n_z

    weights_copy(0, 1, peer(0, 1), source(0, 1)).wait_recv()
    multiply(z, weights_of(n_z // 2))

    @pl.loop(1, n_z // 2)
    def _(k):
        multiply(weights_of(n_z // 2 - k), weights_of(n_z // 2 + k))

    stores = [
        pltpu.make_async_copy(w_recv.at[:, :, pl.ds(0, hid)], gate_out, local_sems.at[7]),
        pltpu.make_async_copy(w_recv.at[:, :, pl.ds(hid, hid)], linear_out, local_sems.at[8]),
    ]
    for store in stores:
        store.start()

    n_q = a_send.shape[0]
    offsets = (4, 5, 3, 0, 6, 2, 7, 1)
    chunk = n_q // CHUNKS
    span = rows // n_q
    groups = (1, 3, 2)
    others = sorted(
        ((a, b) for a in range(SIDE) for b in range(SIDE) if (a, b) != (0, 0)),
        key=lambda ab: -min(ab[0], SIDE - ab[0]) - min(ab[1], SIDE - ab[1]),
    )

    def q_of(j):
        return (z // 2 + offsets[j]) % n_q

    def active_copy(r, dy_, dx_, to, at):
        i = (r * SIDE + dy_) * SIDE + dx_
        return remote(
            a_send.at[pl.ds(r * chunk, chunk), to[1]],
            a_grid.at[at[0], at[1], pl.ds(r * chunk, chunk)],
            a_ssem.at[i],
            a_rsem.at[i],
            {"tp": to[0] * SIDE + to[1]},
        )

    def ahead(dy_, dx_):
        return (y + dy_) % SIDE, (x + dx_) % SIDE

    def behind(dy_, dx_):
        return (y - dy_ + SIDE) % SIDE, (x - dx_ + SIDE) % SIDE

    for r in range(CHUNKS):
        for j in range(r * chunk, (r + 1) * chunk):
            at = pl.ds(pl.multiple_of(q_of(j) * span, 8), span)
            clamped = jnp.minimum(acc[at, 0:hid], clamp_limit)
            linear = jnp.clip(acc[at, hid : 2 * hid], -clamp_limit, clamp_limit)
            active = clamped * jax.nn.sigmoid(gate_slope * clamped) * (linear + 1.0)
            a_send[j] = active.astype(BF).reshape(a_send.shape[1:])
        for dy_, dx_ in others:
            active_copy(r, dy_, dx_, ahead(dy_, dx_), (y, x)).start()
    a_grid[y, x] = a_send[:, x]
    share = chunk * span // SIDE
    for k in (0,) + groups:
        dx.last(k)

    def multiply_down(r):
        at = pl.ds(r * chunk, chunk)
        total = jnp.zeros((share, d_grid.shape[2]), F32)
        for p in range(SIDE):
            total = total + lax.dot_general(
                jnp.concatenate([a_grid[p, g, at].reshape(share, hid) for g in range(SIDE)], axis=1),
                jnp.concatenate([d_grid[p, g] for g in range(SIDE)], axis=1),
                (((1,), (1,)), ((), ())),
                preferred_element_type=F32,
            )
        return total

    def return_copy(j, p):
        to = q_of(j) * SIDE + x
        return remote(
            r_send.at[p, j],
            r_recv.at[f],
            r_ssem.at[j * SIDE + p],
            r_rsem.at[f],
            {"fs": to, "tp": y * SIDE + p},
        ), jnp.logical_and(to == f, p == x)

    def each_return(r, act):
        for j in range(r * chunk, (r + 1) * chunk):
            for p in range(SIDE):
                c, local = return_copy(j, p)
                if offsets[j] != 0:
                    act(c)
                else:

                    @pl.when(jnp.logical_not(local))
                    def _():
                        act(c)

    for r in range(CHUNKS):
        for dy_, dx_ in others:
            active_copy(r, dy_, dx_, ahead(dy_, dx_), behind(dy_, dx_)).wait_recv()
        total = multiply_down(r)
        for p in range(SIDE):
            part = total[:, p * fcols : (p + 1) * fcols].astype(BF)
            r_send[p, pl.ds(r * chunk, chunk)] = part.reshape(chunk, *r_send.shape[2:])
        each_return(r, lambda c: c.start())

    @pl.when(f % SIDE == x)
    def _():
        r_recv[f] = r_send[x, offsets.index(0)]

    drain_all(tokens_copy)
    drain_all(weights_copy)
    for k in groups:
        down_y(k, y).wait_send()
    dx.drain()
    tg.drain()
    for r in range(CHUNKS):
        for dy_, dx_ in others:
            active_copy(r, dy_, dx_, ahead(dy_, dx_), (y, x)).wait_send()
    for store in stores:
        store.wait()

    @pl.loop(0, n_fs)
    def _(e):
        @pl.when(jnp.logical_not(jnp.logical_and(e == f, f % SIDE == x)))
        def _():
            remote(
                r_send.at[0, 0],
                r_recv.at[e],
                r_ssem.at[0],
                r_rsem.at[e],
                {"fs": e, "tp": y * SIDE + f % SIDE},
            ).wait_recv()

    back = r_recv[...].reshape(rows, fcols)
    mix = jnp.dot(high_v[...], back, preferred_element_type=F32) + jnp.dot(
        low_v[...], back, preferred_element_type=F32
    )
    mix_out[...] = mix.astype(BF)
    for r in range(CHUNKS):
        each_return(r, lambda c: c.wait_send())


def copy_out(a, b, c, a_out, b_out, c_out, sems):
    copies = [
        pltpu.make_async_copy(src, dst, sems.at[i])
        for i, (src, dst) in enumerate(((a, a_out), (b, b_out), (c, c_out)))
    ]
    for copy in copies:
        copy.start()
    for copy in copies:
        copy.wait()


def on_device(n_fs, n_tp, tokens, experts, routing, gain, gate_master, linear_master, down_weight):
    tok, top = experts.shape
    ecount, stripe, hid = gate_master.shape
    width = tokens.shape[1]
    fcols = width // n_tp
    cap = 3 * tok * top // (2 * ecount)
    tiles = ecount * cap // 8
    rows = ecount * cap
    vmem, any_space = pl.BlockSpec(memory_space=pltpu.VMEM), pl.BlockSpec(memory_space=pl.ANY)
    hbm = pl.BlockSpec(memory_space=pltpu.HBM)
    sources = ecount // SIDE
    dma = pltpu.SemaphoreType.DMA
    gate_out, linear_out, mix = pl.pallas_call(
        functools.partial(kernel, n_fs, n_tp),
        out_shape=(
            jax.ShapeDtypeStruct((ecount, stripe, hid), BF),
            jax.ShapeDtypeStruct((ecount, stripe, hid), BF),
            jax.ShapeDtypeStruct((tok, fcols), BF),
        ),
        in_specs=[hbm] * 7,
        out_specs=(any_space, any_space, vmem),
        scratch_shapes=[
            pltpu.VMEM((top, tok), jnp.int32),
            pltpu.VMEM((top, tok), F32),
            pltpu.VMEM((width // hid, hid), F32),
            pltpu.VMEM((ecount, stripe, hid), F32),
            pltpu.VMEM((ecount, stripe, hid), F32),
            pltpu.VMEM((tok, fcols), BF),
            pltpu.VMEM((SIDE, width // SIDE, hid), BF),
            pltpu.VMEM((ecount, stripe, 2 * hid), BF),
            pltpu.VMEM((ecount, stripe, 2 * hid), BF),
            pltpu.VMEM((tiles, 8, fcols), BF),
            pltpu.VMEM((n_tp, tiles, 8, fcols), BF),
            pltpu.VMEM((sources, SIDE, cap // 8, 8, hid), BF),
            pltpu.VMEM((SIDE, SIDE, sources, cap // 8, 8, hid), BF),
            pltpu.VMEM((SIDE, SIDE, width // SIDE, hid), BF),
            pltpu.VMEM((SIDE, sources, cap // 8, 8, fcols), BF),
            pltpu.VMEM((ecount, cap // 8, 8, fcols), BF),
            pltpu.VMEM((ecount, tok), F32),
            pltpu.VMEM((ecount, tok), F32),
            pltpu.VMEM((rows, tok), F32),
            pltpu.VMEM((rows, tok), F32),
            pltpu.VMEM((tok, rows), BF),
            pltpu.VMEM((tok, rows), BF),
            pltpu.VMEM((rows, 2 * hid), F32),
            dma((9,)),
            dma((n_fs,)),
            dma((n_fs,)),
            dma((n_fs,)),
            dma((n_fs,)),
            dma((n_fs,)),
            dma((n_fs,)),
            dma((SIDE,)),
            dma((SIDE,)),
            dma((16,)),
            dma((16,)),
            dma((40,)),
            dma((40,)),
            dma((CHUNKS * n_tp,)),
            dma((CHUNKS * n_tp,)),
        ],
        compiler_params=pltpu.CompilerParams(
            collective_id=0, has_side_effects=True, vmem_limit_bytes=48 * 1024 * 1024
        ),
    )(
        *[
            pltpu.with_memory_space_constraint(v, pltpu.HBM)
            for v in (
                experts.T,
                routing.T,
                gain.reshape(width // hid, hid),
                tokens,
                gate_master,
                linear_master,
                down_weight.reshape(SIDE, width // SIDE, hid),
            )
        ]
    )
    shape = (1, width, hid)
    results = (gate_out.reshape(shape), linear_out.reshape(shape), mix)
    return pl.pallas_call(
        copy_out,
        out_shape=tuple(jax.ShapeDtypeStruct(v.shape, v.dtype) for v in results),
        in_specs=[vmem] * 3,
        out_specs=(hbm,) * 3,
        scratch_shapes=[dma((3,))],
    )(*[pltpu.with_memory_space_constraint(v, pltpu.VMEM) for v in results])


def solution(mesh):
    n_fs, n_tp = mesh.shape["fs"], mesh.shape["tp"]
    return jax.shard_map(
        functools.partial(on_device, n_fs, n_tp),
        mesh=mesh,
        in_specs=(
            P("fs", None),
            P("fs", None),
            P("fs", None),
            P(),
            P(None, "fs", "tp"),
            P(None, "fs", "tp"),
            P("fs", None, "tp"),
        ),
        out_specs=(P("fs", None, "tp"), P("fs", None, "tp"), P("fs", "tp")),
        check_vma=False,
    )
```

```python
import functools

import jax
import jax.numpy as jnp
from jax import lax
from jax.experimental import pallas as pl
from jax.experimental.pallas import tpu as pltpu
from jax.sharding import PartitionSpec as P

clamp_limit = 7.0
gate_slope = 1.702
BF = jnp.bfloat16
F32 = jnp.float32
MESH = pl.DeviceIdType.MESH
CHUNKS = 4
SIDE = 4


def remote(src, dst, send_sem, recv_sem, device):
    return pltpu.make_async_remote_copy(
        src_ref=src,
        dst_ref=dst,
        send_sem=send_sem,
        recv_sem=recv_sem,
        device_id=device,
        device_id_type=MESH,
    )


class Torus:
    def __init__(self, grid, send_sems, recv_sems, t):
        self.grid, self.send_sems, self.recv_sems = grid, send_sems, recv_sems
        self.y, self.x = t // SIDE, t % SIDE
        tiles = grid.shape[1]
        self.half, self.quarter = tiles // 2, tiles // 4

    def at(self, h, a, b):
        dx, dy = (a, b) if h == 0 else (b, a)
        return ((self.y + dy + SIDE) % SIDE) * SIDE + (self.x + dx + SIDE) % SIDE

    def copy(self, h, slot, a, b, part, to):
        start = h * self.half + (self.quarter if part == 1 else 0)
        size = self.half if part is None else self.quarter
        ref = self.grid.at[self.at(h, a, b), pl.ds(start, size)]
        k = 0 if slot > 5 and slot % 4 > 1 else 1 + h * 12 + (slot if slot < 4 else 4 + slot // 4 * 2 - 2 + slot % 4)
        return remote(ref, ref, self.send_sems.at[0], self.recv_sems.at[k], {"tp": self.at(h, *to)})

    def send(self, h, slot, a, b, part, to):
        self.copy(h, slot, a, b, part, to).start()

    def recv(self, h, slot, a, b, part):
        self.copy(h, slot, a, b, part, (1, 0)).wait_recv()

    def own(self):
        for h in (0, 1):
            self.send(h, 0, 0, 0, None, (1, 0))
            self.send(h, 1, 0, 0, None, (-1, 0))
            self.column(h, 0, 0)

    def column(self, h, i, a):
        self.send(h, 4 + 4 * i, a, 0, None, (0, 1))
        self.send(h, 5 + 4 * i, a, 0, None, (0, -1))

    def turn(self, h, i, a):
        self.recv(h, 4 + 4 * i, a, -1, None)
        self.send(h, 6 + 4 * i, a, -1, 0, (0, 1))
        self.recv(h, 5 + 4 * i, a, 1, None)
        self.send(h, 7 + 4 * i, a, 1, 1, (0, -1))

    def rest(self):
        for h in (0, 1):
            self.recv(h, 0, -1, 0, None)
            self.send(h, 2, -1, 0, 0, (1, 0))
            self.column(h, 1, -1)
            self.recv(h, 1, 1, 0, None)
            self.send(h, 3, 1, 0, 1, (-1, 0))
            self.column(h, 2, 1)
        for h in (0, 1):
            self.turn(h, 0, 0)
        for h in (0, 1):
            self.recv(h, 2, 2, 0, 0)
            self.recv(h, 3, 2, 0, 1)
            self.column(h, 3, 2)
        for h in (0, 1):
            self.turn(h, 1, -1)
            self.turn(h, 2, 1)
        for h in (0, 1):
            self.turn(h, 3, 2)
        self.whole(SIDE).wait_recv()

    def whole(self, blocks):
        ref = self.grid.at[pl.ds(0, blocks)]
        return remote(ref, ref, self.send_sems.at[0], self.recv_sems.at[0], {"tp": self.at(0, 1, 0)})

    def drain(self):
        self.whole(SIDE * SIDE - 1).wait_send()


class Ring:
    def __init__(self, ref_of, device_of, send_sems, recv_sems, pos):
        self.ref_of, self.device_of, self.pos = ref_of, device_of, pos
        self.send_sems, self.recv_sems = send_sems, recv_sems

    def at(self, step):
        return (self.pos + step + SIDE) % SIDE

    def copy(self, item, slot, step, part, to):
        ref = self.ref_of(self.at(step), item, part)
        k = 0 if slot > 1 else 1 + item * 2 + slot
        return remote(
            ref, ref, self.send_sems.at[0], self.recv_sems.at[k], self.device_of(self.at(to))
        )

    def send(self, item, slot, step, part, to):
        self.copy(item, slot, step, part, to).start()

    def first(self, item):
        self.send(item, 0, 0, None, 1)
        self.send(item, 1, 0, None, -1)

    def second(self, item):
        self.copy(item, 0, -1, None, 1).wait_recv()
        self.send(item, 2, -1, 0, 1)
        self.copy(item, 1, 1, None, 1).wait_recv()
        self.send(item, 3, 1, 1, -1)

    def whole(self, ref):
        return remote(
            ref, ref, self.send_sems.at[0], self.recv_sems.at[0], self.device_of(self.at(1))
        )


def kernel(
    n_fs,
    n_tp,
    experts_hbm,
    routing_hbm,
    gain_hbm,
    tokens_hbm,
    gate_hbm,
    linear_hbm,
    down_hbm,
    gate_out,
    linear_out,
    mix_out,
    experts_ref,
    routing_ref,
    gain_ref,
    gate_v,
    linear_v,
    tok_v,
    down_v,
    w_send,
    w_recv,
    t_send,
    t_grid,
    a_send,
    a_grid,
    d_grid,
    d_turned,
    r_send,
    r_recv,
    slot_v,
    weight_v,
    pick_v,
    mixer_v,
    high_v,
    low_v,
    acc,
    local_sems,
    t_ssem,
    t_rsem,
    w_ssem,
    w_rsem,
    r_ssem,
    r_rsem,
    dy_ssem,
    dy_rsem,
    dx_ssem,
    dx_rsem,
    tg_ssem,
    tg_rsem,
    a_ssem,
    a_rsem,
):
    f, t = lax.axis_index("fs"), lax.axis_index("tp")
    n_z = n_fs // 2
    z, c = f // 2, f % 2
    stripe, hid = gate_v.shape[1], gate_v.shape[2]
    fcols = tok_v.shape[1]
    tok = tok_v.shape[0]
    tiles = t_grid.shape[1]
    rows = tiles * 8
    per = tiles // n_fs
    cap = per * 8

    y, x = t // SIDE, t % SIDE
    loads = [
        pltpu.make_async_copy(
            tokens_hbm.at[:, pl.ds(pl.multiple_of(t * fcols, 128), fcols)], tok_v, local_sems.at[0]
        ),
        pltpu.make_async_copy(gate_hbm, gate_v, local_sems.at[1]),
        pltpu.make_async_copy(linear_hbm, linear_v, local_sems.at[2]),
        pltpu.make_async_copy(down_hbm, down_v, local_sems.at[3]),
        pltpu.make_async_copy(experts_hbm, experts_ref, local_sems.at[4]),
        pltpu.make_async_copy(routing_hbm, routing_ref, local_sems.at[5]),
        pltpu.make_async_copy(gain_hbm, gain_ref, local_sems.at[6]),
    ]
    for load in loads:
        load.start()

    barrier = pltpu.get_barrier_semaphore()

    @pl.loop(1, n_fs)
    def _(k):
        pl.semaphore_signal(
            barrier, inc=1, device_id={"fs": (f + k) % n_fs}, device_id_type=MESH
        )

    @pl.loop(1, n_tp)
    def _(k):
        pl.semaphore_signal(
            barrier, inc=1, device_id={"tp": (t + k) % n_tp}, device_id_type=MESH
        )

    loads[4].wait()
    loads[5].wait()
    names = lax.broadcasted_iota(jnp.int32, (n_fs, tok), 0)
    chosen = jnp.zeros((n_fs, tok), F32)
    weight = jnp.zeros((n_fs, tok), F32)
    for k in range(experts_ref.shape[0]):
        hit = experts_ref[k : k + 1, :] == names
        chosen = chosen + jnp.where(hit, 1.0, 0.0)
        weight = weight + jnp.where(hit, routing_ref[k : k + 1, :], 0.0)
    before = jnp.where(
        lax.broadcasted_iota(jnp.int32, (tok, tok), 0)
        < lax.broadcasted_iota(jnp.int32, (tok, tok), 1),
        1.0,
        0.0,
    ).astype(BF)
    rank = jnp.dot(chosen.astype(BF), before, preferred_element_type=F32)
    slot_v[...] = jnp.where(chosen > 0.0, rank, -1.0)
    weight_v[...] = weight
    places = lax.broadcasted_iota(jnp.int32, (cap, tok), 0).astype(F32)

    @pl.loop(0, n_fs)
    def _(e):
        hit = slot_v[pl.ds(e, 1), :] == places
        at = pl.ds(pl.multiple_of(e * cap, 8), cap)
        pick_v[at, :] = jnp.where(hit, 1.0, 0.0)

    loads[0].wait()
    sent = jnp.dot(pick_v[...].astype(BF), tok_v[...], preferred_element_type=F32)
    t_send[...] = sent.astype(BF).reshape(tiles, 8, fcols)

    loads[6].wait()
    here = lax.broadcasted_iota(jnp.int32, (stripe, hid), 0) + (f * stripe) % hid
    lane = lax.broadcasted_iota(jnp.int32, (stripe, hid), 1)
    picked = jnp.where(here == lane, gain_ref[pl.ds((f * stripe) // hid, 1), :], 0.0)
    column = jnp.sum(picked, axis=1, keepdims=True)
    loads[1].wait()
    loads[2].wait()

    @pl.loop(0, n_fs)
    def _(e):
        w_send[e, :, 0:hid] = (gate_v[e] * column).astype(BF)
        w_send[e, :, hid : 2 * hid] = (linear_v[e] * column).astype(BF)

    loads[3].wait()
    pl.semaphore_wait(barrier, n_fs + n_tp - 2)

    def tile_span(i):
        return pl.ds(i * per, per)

    def peer(dz, dc):
        return ((z + dz) % n_z) * 2 + (c + dc) % 2

    def turn(k):
        return (n_z // 2 + (1 - 2 * (k % 2)) * ((k + 1) // 2)) % n_z

    def tokens_copy(k, to, slot, count=1):
        return remote(
            t_send.at[pl.ds(to * per, count * per)],
            t_grid.at[t, pl.ds(slot * per, count * per)],
            t_ssem.at[0],
            t_rsem.at[0],
            {"fs": to if count == 1 else (f + 1) % n_fs},
        )

    def weights_copy(k, to, slot, count=1):
        i = (k + 1) // 2
        src, dst = w_send.at[pl.ds(to, count)], w_recv.at[pl.ds(slot, count)]
        device = to if count == 1 else (f + 1) % n_fs
        return remote(src, dst, w_ssem.at[0], w_rsem.at[i], {"fs": device})

    def start_all(copy, core):
        dc = (core + c) % 2

        @pl.loop(0, n_z - 1)
        def _(k):
            copy(k, peer(turn(k), dc), f).start()

        @pl.when(dc == 1)
        def _():
            copy(n_z - 1, peer(0, 1), f).start()

    def down_y(k, slot):
        to = (y + k) % SIDE
        return remote(
            down_v.at[to], d_grid.at[slot, x], dy_ssem.at[0], dy_rsem.at[k], {"tp": to * SIDE + x}
        )

    def down_ref(p, k, part):
        block = d_grid.at[(y - k + SIDE) % SIDE, p]
        half = d_grid.shape[2] // 2
        return block if part is None else block.at[pl.ds(part * half, half)]

    dx = Ring(down_ref, lambda p: {"tp": y * SIDE + p}, dx_ssem, dx_rsem, x)

    start_all(tokens_copy, 0)
    start_all(tokens_copy, 1)
    start_all(weights_copy, 0)
    start_all(weights_copy, 1)

    for k in (1, 3, 2):
        down_y(k, y).start()
    d_grid[y, x] = down_v[y]
    dx.first(0)

    t_grid[t, tile_span(f)] = t_send[tile_span(f)]
    w_recv[f] = w_send[f]
    @pl.loop(0, n_fs)
    def _(e):
        hit = slot_v[pl.ds(e, 1), :] == places
        at = pl.ds(pl.multiple_of(e * cap, 8), cap)
        mixer_v[at, :] = jnp.where(hit, weight_v[pl.ds(e, 1), :], 0.0)

    for j in range(rows // 128):
        at = slice(j * 128, (j + 1) * 128)
        turned = mixer_v[at, :].T
        high = turned.astype(BF)
        high_v[:, at] = high
        low_v[:, at] = (turned - high.astype(F32)).astype(BF)
    acc[...] = jnp.zeros_like(acc)

    for k in (1, 3, 2):
        down_y(k, (y - k + SIDE) % SIDE).wait_recv()
        dx.first(k)

    tokens_copy(0, 0, 0, n_fs - 1).wait_recv()
    tg = Torus(t_grid, tg_ssem, tg_rsem, t)
    tg.own()
    for k in (0, 1, 3, 2):
        dx.second(k)
    tg.rest()
    dx.whole(d_grid.at[0]).wait_recv()

    @pl.loop(0, SIDE)
    def _(p):
        for g in range(SIDE):
            d_turned[p, g * hid : (g + 1) * hid, :] = d_grid[p, g].T


    def lhs(chip):
        return t_grid[chip].reshape(rows, fcols)

    def rhs(chip):
        return w_recv[pl.ds(chip * 2, 2)].reshape(fcols, 2 * hid)

    def multiply(one, other):
        acc[...] += jnp.dot(
            jnp.concatenate([lhs(one), lhs(other)], axis=1),
            jnp.concatenate([rhs(one), rhs(other)], axis=0),
            preferred_element_type=F32,
        )

    weights_copy(n_z - 1, peer(0, 1), peer(0, 1)).wait_recv()
    weights_copy(0, 0, 0, 2).wait_recv()
    multiply(z, (z + n_z // 2) % n_z)

    @pl.loop(1, n_z // 2)
    def _(k):
        weights_copy(2 * k, 0, 0, 4).wait_recv()
        multiply((z + n_z // 2 + k) % n_z, (z + n_z // 2 - k) % n_z)

    stores = [
        pltpu.make_async_copy(w_recv.at[:, :, pl.ds(0, hid)], gate_out, local_sems.at[7]),
        pltpu.make_async_copy(w_recv.at[:, :, pl.ds(hid, hid)], linear_out, local_sems.at[8]),
    ]
    for store in stores:
        store.start()

    n_q = a_send.shape[0]
    offsets = (4, 5, 3, 6, 2, 1, 7, 0)
    chunk = n_q // CHUNKS
    span = rows // n_q
    groups = (1, 3, 2)
    others = sorted(
        ((a, b) for a in range(SIDE) for b in range(SIDE) if (a, b) != (0, 0)),
        key=lambda ab: -min(ab[0], SIDE - ab[0]) - min(ab[1], SIDE - ab[1]),
    )

    def q_of(j):
        return (z // 2 + offsets[j]) % n_q

    def active_copy(r, to):
        return remote(
            a_send.at[pl.ds(r * chunk, chunk), to % SIDE],
            a_grid.at[t, pl.ds(r * chunk, chunk)],
            a_ssem.at[0],
            a_rsem.at[r],
            {"tp": to},
        )

    def ahead(dy_, dx_):
        return (y + dy_) % SIDE * SIDE + (x + dx_) % SIDE

    def arrived(at):
        ref = a_grid.at[pl.ds(0, n_tp - 1), at]
        return lambda r: remote(ref, ref, a_ssem.at[0], a_rsem.at[r], {"tp": ahead(0, 1)})

    for r in range(CHUNKS):
        for j in range(r * chunk, (r + 1) * chunk):
            at = pl.ds(pl.multiple_of(q_of(j) * span, 8), span)
            clamped = jnp.minimum(acc[at, 0:hid], clamp_limit)
            linear = jnp.clip(acc[at, hid : 2 * hid], -clamp_limit, clamp_limit)
            active = clamped * jax.nn.sigmoid(gate_slope * clamped) * (linear + 1.0)
            a_send[j] = active.astype(BF).reshape(a_send.shape[1:])
        for dy_, dx_ in others:
            active_copy(r, ahead(dy_, dx_)).start()
    a_grid[t] = a_send[:, x]
    share = chunk * span // SIDE

    def multiply_down(r):
        at = pl.ds(r * chunk, chunk)
        total = jnp.zeros((share, d_turned.shape[2]), F32)
        for p in range(SIDE):
            total = total + lax.dot_general(
                jnp.concatenate(
                    [a_grid[p * SIDE + g, at].reshape(share, hid) for g in range(SIDE)], axis=1
                ),
                d_turned[p],
                (((1,), (0,)), ((), ())),
                preferred_element_type=F32,
            )
        return total

    def return_copy(j, p):
        to = q_of(j) * SIDE + x
        return remote(
            r_send.at[p, j],
            r_recv.at[f],
            r_ssem.at[0],
            r_rsem.at[0],
            {"fs": to, "tp": y * SIDE + p},
        ), jnp.logical_and(to == f, p == x)

    def each_return(r, act):
        for j in range(r * chunk, (r + 1) * chunk):
            for p in range(SIDE):
                c, local = return_copy(j, p)
                if offsets[j] != 0:
                    act(c)
                else:

                    @pl.when(jnp.logical_not(local))
                    def _():
                        act(c)

    weights_copy(0, 0, 0, n_fs - 1).wait_send()
    for r in range(CHUNKS):
        arrived(pl.ds(0, chunk))(r).wait_recv()
        total = multiply_down(r)
        for p in range(SIDE):
            part = total[:, p * fcols : (p + 1) * fcols].astype(BF)
            r_send[p, pl.ds(r * chunk, chunk)] = part.reshape(chunk, *r_send.shape[2:])
        each_return(r, lambda c: c.start())

    @pl.when(f % SIDE == x)
    def _():
        r_recv[f] = r_send[x, offsets.index(0)]

    tokens_copy(0, 0, 0, n_fs - 1).wait_send()
    remote(
        down_v.at[pl.ds(1, SIDE - 1)],
        d_grid.at[0, pl.ds(1, SIDE - 1)],
        dy_ssem.at[0],
        dy_rsem.at[1],
        {"tp": ahead(1, 0)},
    ).wait_send()
    dx.whole(d_grid.at[pl.ds(0, SIDE - 1)]).wait_send()
    tg.drain()
    arrived(pl.ds(0, n_q))(0).wait_send()
    for store in stores:
        store.wait()

    def returned(count):
        ref = r_recv.at[pl.ds(0, count)]
        return remote(ref, ref, r_ssem.at[0], r_rsem.at[0], {"fs": (f + 1) % n_fs})

    mine = f % SIDE == x

    @pl.when(mine)
    def _():
        returned(n_fs - 1).wait_recv()

    @pl.when(jnp.logical_not(mine))
    def _():
        returned(n_fs).wait_recv()

    back = r_recv[...].reshape(rows, fcols)
    mix = jnp.dot(high_v[...], back, preferred_element_type=F32) + jnp.dot(
        low_v[...], back, preferred_element_type=F32
    )
    mix_out[...] = mix.astype(BF)

    @pl.when(mine)
    def _():
        returned(n_fs - 1).wait_send()

    @pl.when(jnp.logical_not(mine))
    def _():
        returned(n_fs).wait_send()


def copy_out(a, b, c, a_out, b_out, c_out, sems):
    copies = [
        pltpu.make_async_copy(src, dst, sems.at[i])
        for i, (src, dst) in enumerate(((a, a_out), (b, b_out), (c, c_out)))
    ]
    for copy in copies:
        copy.start()
    for copy in copies:
        copy.wait()


def on_device(n_fs, n_tp, tokens, experts, routing, gain, gate_master, linear_master, down_weight):
    tok, top = experts.shape
    ecount, stripe, hid = gate_master.shape
    width = tokens.shape[1]
    fcols = width // n_tp
    cap = 3 * tok * top // (2 * ecount)
    tiles = ecount * cap // 8
    rows = ecount * cap
    vmem, any_space = pl.BlockSpec(memory_space=pltpu.VMEM), pl.BlockSpec(memory_space=pl.ANY)
    hbm = pl.BlockSpec(memory_space=pltpu.HBM)
    sources = ecount // SIDE
    dma = pltpu.SemaphoreType.DMA
    gate_out, linear_out, mix = pl.pallas_call(
        functools.partial(kernel, n_fs, n_tp),
        out_shape=(
            jax.ShapeDtypeStruct((ecount, stripe, hid), BF),
            jax.ShapeDtypeStruct((ecount, stripe, hid), BF),
            jax.ShapeDtypeStruct((tok, fcols), BF),
        ),
        in_specs=[hbm] * 7,
        out_specs=(any_space, any_space, vmem),
        scratch_shapes=[
            pltpu.VMEM((top, tok), jnp.int32),
            pltpu.VMEM((top, tok), F32),
            pltpu.VMEM((width // hid, hid), F32),
            pltpu.VMEM((ecount, stripe, hid), F32),
            pltpu.VMEM((ecount, stripe, hid), F32),
            pltpu.VMEM((tok, fcols), BF),
            pltpu.VMEM((SIDE, width // SIDE, hid), BF),
            pltpu.VMEM((ecount, stripe, 2 * hid), BF),
            pltpu.VMEM((ecount, stripe, 2 * hid), BF),
            pltpu.VMEM((tiles, 8, fcols), BF),
            pltpu.VMEM((n_tp, tiles, 8, fcols), BF),
            pltpu.VMEM((sources, SIDE, cap // 8, 8, hid), BF),
            pltpu.VMEM((n_tp, sources, cap // 8, 8, hid), BF),
            pltpu.VMEM((SIDE, SIDE, width // SIDE, hid), BF),
            pltpu.VMEM((SIDE, SIDE * hid, width // SIDE), BF),
            pltpu.VMEM((SIDE, sources, cap // 8, 8, fcols), BF),
            pltpu.VMEM((ecount, cap // 8, 8, fcols), BF),
            pltpu.VMEM((ecount, tok), F32),
            pltpu.VMEM((ecount, tok), F32),
            pltpu.VMEM((rows, tok), F32),
            pltpu.VMEM((rows, tok), F32),
            pltpu.VMEM((tok, rows), BF),
            pltpu.VMEM((tok, rows), BF),
            pltpu.VMEM((rows, 2 * hid), F32),
            dma((9,)),
            dma((1,)),
            dma((1,)),
            dma((1,)),
            dma((ecount // 4 + 1,)),
            dma((1,)),
            dma((1,)),
            dma((1,)),
            dma((SIDE,)),
            dma((1,)),
            dma((9,)),
            dma((1,)),
            dma((25,)),
            dma((1,)),
            dma((CHUNKS,)),
        ],
        compiler_params=pltpu.CompilerParams(
            collective_id=0, has_side_effects=True, vmem_limit_bytes=48 * 1024 * 1024
        ),
    )(
        *[
            pltpu.with_memory_space_constraint(v, pltpu.HBM)
            for v in (
                experts.T,
                routing.T,
                gain.reshape(width // hid, hid),
                tokens,
                gate_master,
                linear_master,
                down_weight.reshape(SIDE, width // SIDE, hid),
            )
        ]
    )
    shape = (1, width, hid)
    results = (gate_out.reshape(shape), linear_out.reshape(shape), mix)
    return pl.pallas_call(
        copy_out,
        out_shape=tuple(jax.ShapeDtypeStruct(v.shape, v.dtype) for v in results),
        in_specs=[vmem] * 3,
        out_specs=(hbm,) * 3,
        scratch_shapes=[dma((3,))],
    )(*[pltpu.with_memory_space_constraint(v, pltpu.VMEM) for v in results])


def solution(mesh):
    n_fs, n_tp = mesh.shape["fs"], mesh.shape["tp"]
    return jax.shard_map(
        functools.partial(on_device, n_fs, n_tp),
        mesh=mesh,
        in_specs=(
            P("fs", None),
            P("fs", None),
            P("fs", None),
            P(),
            P(None, "fs", "tp"),
            P(None, "fs", "tp"),
            P("fs", None, "tp"),
        ),
        out_specs=(P("fs", None, "tp"), P("fs", None, "tp"), P("fs", "tp")),
        check_vma=False,
    )
```

```python
import functools

import jax
import jax.numpy as jnp
from jax import lax
from jax.experimental import pallas as pl
from jax.experimental.pallas import tpu as pltpu
from jax.sharding import PartitionSpec as P

clamp_limit = 7.0
gate_slope = 1.702
BF = jnp.bfloat16
F32 = jnp.float32
MESH = pl.DeviceIdType.MESH
CHUNKS = 8
SIDE = 4


def remote(src, dst, send_sem, recv_sem, device):
    return pltpu.make_async_remote_copy(
        src_ref=src,
        dst_ref=dst,
        send_sem=send_sem,
        recv_sem=recv_sem,
        device_id=device,
        device_id_type=MESH,
    )


class Torus:
    def __init__(self, grid, send_sems, recv_sems, t):
        self.grid, self.send_sems, self.recv_sems = grid, send_sems, recv_sems
        self.y, self.x = t // SIDE, t % SIDE
        tiles = grid.shape[1]
        self.half, self.quarter = tiles // 2, tiles // 4

    def at(self, h, a, b):
        dx, dy = (a, b) if h == 0 else (b, a)
        return ((self.y + dy + SIDE) % SIDE) * SIDE + (self.x + dx + SIDE) % SIDE

    def copy(self, h, slot, a, b, part, to):
        start = h * self.half + (self.quarter if part == 1 else 0)
        size = self.half if part is None else self.quarter
        ref = self.grid.at[self.at(h, a, b), pl.ds(start, size)]
        k = 0 if slot > 5 and slot % 4 > 1 else 1 + h * 12 + (slot if slot < 4 else 4 + slot // 4 * 2 - 2 + slot % 4)
        return remote(ref, ref, self.send_sems.at[0], self.recv_sems.at[k], {"tp": self.at(h, *to)})

    def send(self, h, slot, a, b, part, to):
        self.copy(h, slot, a, b, part, to).start()

    def recv(self, h, slot, a, b, part):
        self.copy(h, slot, a, b, part, (1, 0)).wait_recv()

    def own(self):
        for h in (0, 1):
            self.send(h, 0, 0, 0, None, (1, 0))
            self.send(h, 1, 0, 0, None, (-1, 0))
            self.column(h, 0, 0)

    def column(self, h, i, a):
        self.send(h, 4 + 4 * i, a, 0, None, (0, 1))
        self.send(h, 5 + 4 * i, a, 0, None, (0, -1))

    def turn(self, h, i, a):
        self.recv(h, 4 + 4 * i, a, -1, None)
        self.send(h, 6 + 4 * i, a, -1, 0, (0, 1))
        self.recv(h, 5 + 4 * i, a, 1, None)
        self.send(h, 7 + 4 * i, a, 1, 1, (0, -1))

    def rest(self):
        for h in (0, 1):
            self.recv(h, 0, -1, 0, None)
            self.send(h, 2, -1, 0, 0, (1, 0))
            self.column(h, 1, -1)
            self.recv(h, 1, 1, 0, None)
            self.send(h, 3, 1, 0, 1, (-1, 0))
            self.column(h, 2, 1)
        for h in (0, 1):
            self.turn(h, 0, 0)
        for h in (0, 1):
            self.recv(h, 2, 2, 0, 0)
            self.recv(h, 3, 2, 0, 1)
            self.column(h, 3, 2)
        for h in (0, 1):
            self.turn(h, 1, -1)
            self.turn(h, 2, 1)
        for h in (0, 1):
            self.turn(h, 3, 2)
        self.whole(SIDE).wait_recv()

    def whole(self, blocks):
        ref = self.grid.at[pl.ds(0, blocks)]
        return remote(ref, ref, self.send_sems.at[0], self.recv_sems.at[0], {"tp": self.at(0, 1, 0)})

    def drain(self):
        self.whole(SIDE * SIDE - 1).wait_send()


class Ring:
    def __init__(self, ref_of, device_of, send_sems, recv_sems, pos):
        self.ref_of, self.device_of, self.pos = ref_of, device_of, pos
        self.send_sems, self.recv_sems = send_sems, recv_sems

    def at(self, step):
        return (self.pos + step + SIDE) % SIDE

    def copy(self, item, slot, step, part, to):
        ref = self.ref_of(self.at(step), item, part)
        k = 0 if slot > 1 else 1 + item * 2 + slot
        return remote(
            ref, ref, self.send_sems.at[0], self.recv_sems.at[k], self.device_of(self.at(to))
        )

    def send(self, item, slot, step, part, to):
        self.copy(item, slot, step, part, to).start()

    def first(self, item):
        self.send(item, 0, 0, None, 1)
        self.send(item, 1, 0, None, -1)

    def second(self, item):
        self.copy(item, 0, -1, None, 1).wait_recv()
        self.send(item, 2, -1, 0, 1)
        self.copy(item, 1, 1, None, 1).wait_recv()
        self.send(item, 3, 1, 1, -1)

    def whole(self, ref):
        return remote(
            ref, ref, self.send_sems.at[0], self.recv_sems.at[0], self.device_of(self.at(1))
        )


def kernel(
    n_fs,
    n_tp,
    experts_hbm,
    routing_hbm,
    gain_hbm,
    tokens_hbm,
    gate_hbm,
    linear_hbm,
    down_hbm,
    gate_out,
    linear_out,
    mix_out,
    experts_ref,
    routing_ref,
    gain_ref,
    gate_v,
    linear_v,
    tok_v,
    down_v,
    w_send,
    w_recv,
    t_send,
    t_grid,
    t_rows,
    a_send,
    a_grid,
    d_grid,
    d_turned,
    r_send,
    r_recv,
    slot_v,
    weight_v,
    pick_v,
    mixer_v,
    high_v,
    low_v,
    acc,
    local_sems,
    t_ssem,
    t_rsem,
    w_ssem,
    w_rsem,
    r_ssem,
    r_rsem,
    dy_ssem,
    dy_rsem,
    dx_ssem,
    dx_rsem,
    tg_ssem,
    tg_rsem,
    a_ssem,
    a_rsem,
):
    f, t = lax.axis_index("fs"), lax.axis_index("tp")
    n_z = n_fs // 2
    z, c = f // 2, f % 2
    stripe, hid = gate_v.shape[1], gate_v.shape[2]
    fcols = tok_v.shape[1]
    tok = tok_v.shape[0]
    tiles = t_grid.shape[1]
    rows = tiles * 8
    per = tiles // n_fs
    cap = per * 8

    y, x = t // SIDE, t % SIDE
    loads = [
        pltpu.make_async_copy(
            tokens_hbm.at[:, pl.ds(pl.multiple_of(t * fcols, 128), fcols)], tok_v, local_sems.at[0]
        ),
        pltpu.make_async_copy(gate_hbm, gate_v, local_sems.at[1]),
        pltpu.make_async_copy(linear_hbm, linear_v, local_sems.at[2]),
        pltpu.make_async_copy(down_hbm, down_v, local_sems.at[3]),
        pltpu.make_async_copy(experts_hbm, experts_ref, local_sems.at[4]),
        pltpu.make_async_copy(routing_hbm, routing_ref, local_sems.at[5]),
        pltpu.make_async_copy(gain_hbm, gain_ref, local_sems.at[6]),
    ]
    for load in loads:
        load.start()

    barrier = pltpu.get_barrier_semaphore()

    @pl.loop(1, n_fs)
    def _(k):
        pl.semaphore_signal(
            barrier, inc=1, device_id={"fs": (f + k) % n_fs}, device_id_type=MESH
        )

    @pl.loop(1, n_tp)
    def _(k):
        pl.semaphore_signal(
            barrier, inc=1, device_id={"tp": (t + k) % n_tp}, device_id_type=MESH
        )

    loads[4].wait()
    loads[5].wait()
    names = lax.broadcasted_iota(jnp.int32, (n_fs, tok), 0)
    chosen = jnp.zeros((n_fs, tok), F32)
    weight = jnp.zeros((n_fs, tok), F32)
    for k in range(experts_ref.shape[0]):
        hit = experts_ref[k : k + 1, :] == names
        chosen = chosen + jnp.where(hit, 1.0, 0.0)
        weight = weight + jnp.where(hit, routing_ref[k : k + 1, :], 0.0)
    before = jnp.where(
        lax.broadcasted_iota(jnp.int32, (tok, tok), 0)
        < lax.broadcasted_iota(jnp.int32, (tok, tok), 1),
        1.0,
        0.0,
    ).astype(BF)
    rank = jnp.dot(chosen.astype(BF), before, preferred_element_type=F32)
    slot_v[...] = jnp.where(chosen > 0.0, rank, -1.0)
    weight_v[...] = weight
    places = lax.broadcasted_iota(jnp.int32, (cap, tok), 0).astype(F32)

    @pl.loop(0, n_fs)
    def _(e):
        hit = slot_v[pl.ds(e, 1), :] == places
        at = pl.ds(pl.multiple_of(e * cap, 8), cap)
        pick_v[at, :] = jnp.where(hit, 1.0, 0.0)

    loads[0].wait()
    sent = jnp.dot(pick_v[...].astype(BF), tok_v[...], preferred_element_type=F32)
    t_send[...] = sent.astype(BF).reshape(tiles, 8, fcols)

    loads[6].wait()
    here = lax.broadcasted_iota(jnp.int32, (stripe, hid), 0) + (f * stripe) % hid
    lane = lax.broadcasted_iota(jnp.int32, (stripe, hid), 1)
    picked = jnp.where(here == lane, gain_ref[pl.ds((f * stripe) // hid, 1), :], 0.0)
    column = jnp.sum(picked, axis=1, keepdims=True)
    loads[1].wait()
    loads[2].wait()

    @pl.loop(0, n_fs)
    def _(e):
        w_send[e, :, 0:hid] = (gate_v[e] * column).astype(BF)
        w_send[e, :, hid : 2 * hid] = (linear_v[e] * column).astype(BF)

    loads[3].wait()
    pl.semaphore_wait(barrier, n_fs + n_tp - 2)

    def tile_span(i):
        return pl.ds(i * per, per)

    def peer(dz, dc):
        return ((z + dz) % n_z) * 2 + (c + dc) % 2

    def turn(k):
        return (n_z // 2 + (1 - 2 * (k % 2)) * ((k + 1) // 2)) % n_z

    def tokens_copy(k, to, slot, count=1):
        return remote(
            t_send.at[pl.ds(to * per, count * per)],
            t_grid.at[t, pl.ds(slot * per, count * per)],
            t_ssem.at[0],
            t_rsem.at[0],
            {"fs": to if count == 1 else (f + 1) % n_fs},
        )

    def weights_copy(k, to, slot, count=1):
        i = (k + 1) // 2
        src, dst = w_send.at[pl.ds(to, count)], w_recv.at[pl.ds(slot, count)]
        device = to if count == 1 else (f + 1) % n_fs
        return remote(src, dst, w_ssem.at[0], w_rsem.at[i], {"fs": device})

    def start_all(copy, core):
        dc = (core + c) % 2

        @pl.loop(0, n_z - 1)
        def _(k):
            copy(k, peer(turn(k), dc), f).start()

        @pl.when(dc == 1)
        def _():
            copy(n_z - 1, peer(0, 1), f).start()

    def down_y(k, slot):
        to = (y + k) % SIDE
        return remote(
            down_v.at[to], d_grid.at[slot, x], dy_ssem.at[0], dy_rsem.at[k], {"tp": to * SIDE + x}
        )

    def down_ref(p, k, part):
        block = d_grid.at[(y - k + SIDE) % SIDE, p]
        half = d_grid.shape[2] // 2
        return block if part is None else block.at[pl.ds(part * half, half)]

    dx = Ring(down_ref, lambda p: {"tp": y * SIDE + p}, dx_ssem, dx_rsem, x)

    start_all(tokens_copy, 0)
    start_all(tokens_copy, 1)
    start_all(weights_copy, 0)
    start_all(weights_copy, 1)

    for k in (1, 3, 2):
        down_y(k, y).start()
    d_grid[y, x] = down_v[y]
    dx.first(0)

    t_grid[t, tile_span(f)] = t_send[tile_span(f)]
    w_recv[f] = w_send[f]
    @pl.loop(0, n_fs)
    def _(e):
        hit = slot_v[pl.ds(e, 1), :] == places
        at = pl.ds(pl.multiple_of(e * cap, 8), cap)
        mixer_v[at, :] = jnp.where(hit, weight_v[pl.ds(e, 1), :], 0.0)

    for j in range(rows // 128):
        at = slice(j * 128, (j + 1) * 128)
        turned = mixer_v[at, :].T
        high = turned.astype(BF)
        high_v[:, at] = high
        low_v[:, at] = (turned - high.astype(F32)).astype(BF)
    acc[...] = jnp.zeros_like(acc)

    for k in (1, 3, 2):
        down_y(k, (y - k + SIDE) % SIDE).wait_recv()
        dx.first(k)

    tokens_copy(0, 0, 0, n_fs - 1).wait_recv()
    tg = Torus(t_grid, tg_ssem, tg_rsem, t)
    tg.own()
    for k in (0, 1, 3, 2):
        dx.second(k)
    tg.rest()
    dx.whole(d_grid.at[0]).wait_recv()

    @pl.loop(0, n_tp)
    def _(b):
        t_rows[b] = t_grid[b].reshape(rows, fcols)

    @pl.loop(0, SIDE)
    def _(p):
        for g in range(SIDE):
            d_turned[p, g * hid : (g + 1) * hid, :] = d_grid[p, g].T


    def lhs(chip):
        return t_rows[chip]

    def rhs(chip):
        return w_recv[pl.ds(chip * 2, 2)].reshape(fcols, 2 * hid)

    def multiply(one, other):
        acc[...] += jnp.dot(
            jnp.concatenate([lhs(one), lhs(other)], axis=1),
            jnp.concatenate([rhs(one), rhs(other)], axis=0),
            preferred_element_type=F32,
        )

    weights_copy(n_z - 1, peer(0, 1), peer(0, 1)).wait_recv()
    weights_copy(0, 0, 0, 2).wait_recv()
    multiply(z, (z + n_z // 2) % n_z)

    @pl.loop(1, n_z // 2)
    def _(k):
        weights_copy(2 * k, 0, 0, 4).wait_recv()
        multiply((z + n_z // 2 + k) % n_z, (z + n_z // 2 - k) % n_z)

    stores = [
        pltpu.make_async_copy(w_recv.at[:, :, pl.ds(0, hid)], gate_out, local_sems.at[7]),
        pltpu.make_async_copy(w_recv.at[:, :, pl.ds(hid, hid)], linear_out, local_sems.at[8]),
    ]
    for store in stores:
        store.start()

    n_q = a_send.shape[0]
    offsets = (4, 5, 3, 6, 2, 1, 7, 0)
    chunk = n_q // CHUNKS
    span = rows // n_q
    groups = (1, 3, 2)
    others = sorted(
        ((a, b) for a in range(SIDE) for b in range(SIDE) if (a, b) != (0, 0)),
        key=lambda ab: -min(ab[0], SIDE - ab[0]) - min(ab[1], SIDE - ab[1]),
    )

    def q_of(j):
        return (z // 2 + offsets[j]) % n_q

    def active_copy(r, to):
        return remote(
            a_send.at[pl.ds(r * chunk, chunk), to % SIDE],
            a_grid.at[t, pl.ds(r * chunk, chunk)],
            a_ssem.at[0],
            a_rsem.at[r],
            {"tp": to},
        )

    def ahead(dy_, dx_):
        return (y + dy_) % SIDE * SIDE + (x + dx_) % SIDE

    def arrived(at):
        ref = a_grid.at[pl.ds(0, n_tp - 1), at]
        return lambda r: remote(ref, ref, a_ssem.at[0], a_rsem.at[r], {"tp": ahead(0, 1)})

    for r in range(CHUNKS):
        for j in range(r * chunk, (r + 1) * chunk):
            at = pl.ds(pl.multiple_of(q_of(j) * span, 8), span)
            clamped = jnp.minimum(acc[at, 0:hid], clamp_limit)
            linear = jnp.clip(acc[at, hid : 2 * hid], -clamp_limit, clamp_limit)
            active = clamped * jax.nn.sigmoid(gate_slope * clamped) * (linear + 1.0)
            a_send[j] = active.astype(BF).reshape(a_send.shape[1:])
        for dy_, dx_ in others:
            active_copy(r, ahead(dy_, dx_)).start()
    a_grid[t] = a_send[:, x]
    share = chunk * span // SIDE

    def multiply_down(r):
        at = pl.ds(r * chunk, chunk)
        total = jnp.zeros((share, d_turned.shape[2]), F32)
        for p in range(SIDE):
            total = total + lax.dot_general(
                jnp.concatenate(
                    [a_grid[p * SIDE + g, at].reshape(share, hid) for g in range(SIDE)], axis=1
                ),
                d_turned[p],
                (((1,), (0,)), ((), ())),
                preferred_element_type=F32,
            )
        return total

    def return_copy(j, p):
        to = q_of(j) * SIDE + x
        return remote(
            r_send.at[p, j],
            r_recv.at[f],
            r_ssem.at[0],
            r_rsem.at[0],
            {"fs": to, "tp": y * SIDE + p},
        ), jnp.logical_and(to == f, p == x)

    def each_return(r, act):
        for j in range(r * chunk, (r + 1) * chunk):
            for p in range(SIDE):
                c, local = return_copy(j, p)
                if offsets[j] != 0:
                    act(c)
                else:

                    @pl.when(jnp.logical_not(local))
                    def _():
                        act(c)

    weights_copy(0, 0, 0, n_fs - 1).wait_send()
    for r in range(CHUNKS):
        arrived(pl.ds(0, chunk))(r).wait_recv()
        total = multiply_down(r)
        for p in range(SIDE):
            part = total[:, p * fcols : (p + 1) * fcols].astype(BF)
            r_send[p, pl.ds(r * chunk, chunk)] = part.reshape(chunk, *r_send.shape[2:])
        each_return(r, lambda c: c.start())

    @pl.when(f % SIDE == x)
    def _():
        r_recv[f] = r_send[x, offsets.index(0)]

    tokens_copy(0, 0, 0, n_fs - 1).wait_send()
    remote(
        down_v.at[pl.ds(1, SIDE - 1)],
        d_grid.at[0, pl.ds(1, SIDE - 1)],
        dy_ssem.at[0],
        dy_rsem.at[1],
        {"tp": ahead(1, 0)},
    ).wait_send()
    dx.whole(d_grid.at[pl.ds(0, SIDE - 1)]).wait_send()
    tg.drain()
    arrived(pl.ds(0, n_q))(0).wait_send()
    for store in stores:
        store.wait()

    def returned(count):
        ref = r_recv.at[pl.ds(0, count)]
        return remote(ref, ref, r_ssem.at[0], r_rsem.at[0], {"fs": (f + 1) % n_fs})

    mine = f % SIDE == x

    @pl.when(mine)
    def _():
        returned(n_fs - 1).wait_recv()

    @pl.when(jnp.logical_not(mine))
    def _():
        returned(n_fs).wait_recv()

    back = r_recv[...].reshape(rows, fcols)
    mix = jnp.dot(high_v[...], back, preferred_element_type=F32) + jnp.dot(
        low_v[...], back, preferred_element_type=F32
    )
    mix_out[...] = mix.astype(BF)

    @pl.when(mine)
    def _():
        returned(n_fs - 1).wait_send()

    @pl.when(jnp.logical_not(mine))
    def _():
        returned(n_fs).wait_send()


def copy_out(a, b, c, a_out, b_out, c_out, sems):
    copies = [
        pltpu.make_async_copy(src, dst, sems.at[i])
        for i, (src, dst) in enumerate(((a, a_out), (b, b_out), (c, c_out)))
    ]
    for copy in copies:
        copy.start()
    for copy in copies:
        copy.wait()


def on_device(n_fs, n_tp, tokens, experts, routing, gain, gate_master, linear_master, down_weight):
    tok, top = experts.shape
    ecount, stripe, hid = gate_master.shape
    width = tokens.shape[1]
    fcols = width // n_tp
    cap = 3 * tok * top // (2 * ecount)
    tiles = ecount * cap // 8
    rows = ecount * cap
    vmem, any_space = pl.BlockSpec(memory_space=pltpu.VMEM), pl.BlockSpec(memory_space=pl.ANY)
    hbm = pl.BlockSpec(memory_space=pltpu.HBM)
    sources = ecount // SIDE
    dma = pltpu.SemaphoreType.DMA
    gate_out, linear_out, mix = pl.pallas_call(
        functools.partial(kernel, n_fs, n_tp),
        out_shape=(
            jax.ShapeDtypeStruct((ecount, stripe, hid), BF),
            jax.ShapeDtypeStruct((ecount, stripe, hid), BF),
            jax.ShapeDtypeStruct((tok, fcols), BF),
        ),
        in_specs=[hbm] * 7,
        out_specs=(any_space, any_space, vmem),
        scratch_shapes=[
            pltpu.VMEM((top, tok), jnp.int32),
            pltpu.VMEM((top, tok), F32),
            pltpu.VMEM((width // hid, hid), F32),
            pltpu.VMEM((ecount, stripe, hid), F32),
            pltpu.VMEM((ecount, stripe, hid), F32),
            pltpu.VMEM((tok, fcols), BF),
            pltpu.VMEM((SIDE, width // SIDE, hid), BF),
            pltpu.VMEM((ecount, stripe, 2 * hid), BF),
            pltpu.VMEM((ecount, stripe, 2 * hid), BF),
            pltpu.VMEM((tiles, 8, fcols), BF),
            pltpu.VMEM((n_tp, tiles, 8, fcols), BF),
            pltpu.VMEM((n_tp, rows, fcols), BF),
            pltpu.VMEM((sources, SIDE, cap // 8, 8, hid), BF),
            pltpu.VMEM((n_tp, sources, cap // 8, 8, hid), BF),
            pltpu.VMEM((SIDE, SIDE, width // SIDE, hid), BF),
            pltpu.VMEM((SIDE, SIDE * hid, width // SIDE), BF),
            pltpu.VMEM((SIDE, sources, cap // 8, 8, fcols), BF),
            pltpu.VMEM((ecount, cap // 8, 8, fcols), BF),
            pltpu.VMEM((ecount, tok), F32),
            pltpu.VMEM((ecount, tok), F32),
            pltpu.VMEM((rows, tok), F32),
            pltpu.VMEM((rows, tok), F32),
            pltpu.VMEM((tok, rows), BF),
            pltpu.VMEM((tok, rows), BF),
            pltpu.VMEM((rows, 2 * hid), F32),
            dma((9,)),
            dma((1,)),
            dma((1,)),
            dma((1,)),
            dma((ecount // 4 + 1,)),
            dma((1,)),
            dma((1,)),
            dma((1,)),
            dma((SIDE,)),
            dma((1,)),
            dma((9,)),
            dma((1,)),
            dma((25,)),
            dma((1,)),
            dma((CHUNKS,)),
        ],
        compiler_params=pltpu.CompilerParams(
            collective_id=0, has_side_effects=True, vmem_limit_bytes=48 * 1024 * 1024
        ),
    )(
        *[
            pltpu.with_memory_space_constraint(v, pltpu.HBM)
            for v in (
                experts.T,
                routing.T,
                gain.reshape(width // hid, hid),
                tokens,
                gate_master,
                linear_master,
                down_weight.reshape(SIDE, width // SIDE, hid),
            )
        ]
    )
    shape = (1, width, hid)
    results = (gate_out.reshape(shape), linear_out.reshape(shape), mix)
    return pl.pallas_call(
        copy_out,
        out_shape=tuple(jax.ShapeDtypeStruct(v.shape, v.dtype) for v in results),
        in_specs=[vmem] * 3,
        out_specs=(hbm,) * 3,
        scratch_shapes=[dma((3,))],
    )(*[pltpu.with_memory_space_constraint(v, pltpu.VMEM) for v in results])


def solution(mesh):
    n_fs, n_tp = mesh.shape["fs"], mesh.shape["tp"]
    return jax.shard_map(
        functools.partial(on_device, n_fs, n_tp),
        mesh=mesh,
        in_specs=(
            P("fs", None),
            P("fs", None),
            P("fs", None),
            P(),
            P(None, "fs", "tp"),
            P(None, "fs", "tp"),
            P("fs", None, "tp"),
        ),
        out_specs=(P("fs", None, "tp"), P("fs", None, "tp"), P("fs", "tp")),
        check_vma=False,
    )
```

```python
import functools

import jax
import jax.numpy as jnp
from jax import lax
from jax.experimental import pallas as pl
from jax.experimental.pallas import tpu as pltpu
from jax.sharding import PartitionSpec as P

clamp_limit = 7.0
gate_slope = 1.702
BF = jnp.bfloat16
F32 = jnp.float32
MESH = pl.DeviceIdType.MESH
CHUNKS = 8
SIDE = 4


def remote(src, dst, send_sem, recv_sem, device):
    return pltpu.make_async_remote_copy(
        src_ref=src,
        dst_ref=dst,
        send_sem=send_sem,
        recv_sem=recv_sem,
        device_id=device,
        device_id_type=MESH,
    )


class Torus:
    def __init__(self, grid, send_sems, recv_sems, t):
        self.grid, self.send_sems, self.recv_sems = grid, send_sems, recv_sems
        self.y, self.x = t // SIDE, t % SIDE
        tiles = grid.shape[1]
        self.half, self.quarter = tiles // 2, tiles // 4

    def at(self, h, a, b):
        dx, dy = (a, b) if h == 0 else (b, a)
        return ((self.y + dy + SIDE) % SIDE) * SIDE + (self.x + dx + SIDE) % SIDE

    def copy(self, h, slot, a, b, part, to):
        start = h * self.half + (self.quarter if part == 1 else 0)
        size = self.half if part is None else self.quarter
        ref = self.grid.at[self.at(h, a, b), pl.ds(start, size)]
        k = 0 if slot > 5 and slot % 4 > 1 else 1 + h * 12 + (slot if slot < 4 else 4 + slot // 4 * 2 - 2 + slot % 4)
        return remote(ref, ref, self.send_sems.at[0], self.recv_sems.at[k], {"tp": self.at(h, *to)})

    def send(self, h, slot, a, b, part, to):
        self.copy(h, slot, a, b, part, to).start()

    def recv(self, h, slot, a, b, part):
        self.copy(h, slot, a, b, part, (1, 0)).wait_recv()

    def own(self):
        for h in (0, 1):
            self.send(h, 0, 0, 0, None, (1, 0))
            self.send(h, 1, 0, 0, None, (-1, 0))
            self.column(h, 0, 0)

    def column(self, h, i, a):
        self.send(h, 4 + 4 * i, a, 0, None, (0, 1))
        self.send(h, 5 + 4 * i, a, 0, None, (0, -1))

    def turn(self, h, i, a):
        self.recv(h, 4 + 4 * i, a, -1, None)
        self.send(h, 6 + 4 * i, a, -1, 0, (0, 1))
        self.recv(h, 5 + 4 * i, a, 1, None)
        self.send(h, 7 + 4 * i, a, 1, 1, (0, -1))

    def rest(self):
        for h in (0, 1):
            self.recv(h, 0, -1, 0, None)
            self.send(h, 2, -1, 0, 0, (1, 0))
            self.column(h, 1, -1)
            self.recv(h, 1, 1, 0, None)
            self.send(h, 3, 1, 0, 1, (-1, 0))
            self.column(h, 2, 1)
        for h in (0, 1):
            self.turn(h, 0, 0)
        for h in (0, 1):
            self.recv(h, 2, 2, 0, 0)
            self.recv(h, 3, 2, 0, 1)
            self.column(h, 3, 2)
        for h in (0, 1):
            self.turn(h, 1, -1)
            self.turn(h, 2, 1)
        for h in (0, 1):
            self.turn(h, 3, 2)
        self.whole(SIDE).wait_recv()

    def whole(self, blocks):
        ref = self.grid.at[pl.ds(0, blocks)]
        return remote(ref, ref, self.send_sems.at[0], self.recv_sems.at[0], {"tp": self.at(0, 1, 0)})

    def drain(self):
        self.whole(SIDE * SIDE - 1).wait_send()


class Ring:
    def __init__(self, ref_of, device_of, send_sems, recv_sems, pos):
        self.ref_of, self.device_of, self.pos = ref_of, device_of, pos
        self.send_sems, self.recv_sems = send_sems, recv_sems

    def at(self, step):
        return (self.pos + step + SIDE) % SIDE

    def copy(self, item, slot, step, part, to):
        ref = self.ref_of(self.at(step), item, part)
        k = 0 if slot > 1 else 1 + item * 2 + slot
        return remote(
            ref, ref, self.send_sems.at[0], self.recv_sems.at[k], self.device_of(self.at(to))
        )

    def send(self, item, slot, step, part, to):
        self.copy(item, slot, step, part, to).start()

    def first(self, item):
        self.send(item, 0, 0, None, 1)
        self.send(item, 1, 0, None, -1)

    def second(self, item):
        self.copy(item, 0, -1, None, 1).wait_recv()
        self.send(item, 2, -1, 0, 1)
        self.copy(item, 1, 1, None, 1).wait_recv()
        self.send(item, 3, 1, 1, -1)

    def whole(self, ref):
        return remote(
            ref, ref, self.send_sems.at[0], self.recv_sems.at[0], self.device_of(self.at(1))
        )


def kernel(
    n_fs,
    n_tp,
    experts_hbm,
    routing_hbm,
    gain_hbm,
    tokens_hbm,
    gate_hbm,
    linear_hbm,
    down_hbm,
    gate_out,
    linear_out,
    mix_out,
    experts_ref,
    routing_ref,
    gain_ref,
    gate_v,
    linear_v,
    tok_v,
    down_v,
    w_send,
    w_recv,
    t_send,
    t_grid,
    t_rows,
    a_send,
    a_grid,
    d_grid,
    d_turned,
    r_send,
    r_recv,
    slot_v,
    weight_v,
    pick_v,
    mixer_v,
    high_v,
    low_v,
    acc,
    local_sems,
    t_ssem,
    t_rsem,
    w_ssem,
    w_rsem,
    r_ssem,
    r_rsem,
    dy_ssem,
    dy_rsem,
    dx_ssem,
    dx_rsem,
    tg_ssem,
    tg_rsem,
    a_ssem,
    a_rsem,
):
    f, t = lax.axis_index("fs"), lax.axis_index("tp")
    n_z = n_fs // 2
    z, c = f // 2, f % 2
    stripe, hid = gate_v.shape[1], gate_v.shape[2]
    fcols = tok_v.shape[1]
    tok = tok_v.shape[0]
    tiles = t_grid.shape[1]
    rows = tiles * 8
    per = tiles // n_fs
    cap = per * 8

    y, x = t // SIDE, t % SIDE
    loads = [
        pltpu.make_async_copy(
            tokens_hbm.at[:, pl.ds(pl.multiple_of(t * fcols, 128), fcols)], tok_v, local_sems.at[0]
        ),
        pltpu.make_async_copy(gate_hbm, gate_v, local_sems.at[1]),
        pltpu.make_async_copy(linear_hbm, linear_v, local_sems.at[2]),
        pltpu.make_async_copy(down_hbm, down_v, local_sems.at[3]),
        pltpu.make_async_copy(experts_hbm, experts_ref, local_sems.at[4]),
        pltpu.make_async_copy(routing_hbm, routing_ref, local_sems.at[5]),
        pltpu.make_async_copy(gain_hbm, gain_ref, local_sems.at[6]),
    ]
    for load in loads:
        load.start()

    barrier = pltpu.get_barrier_semaphore()

    @pl.loop(1, n_fs)
    def _(k):
        pl.semaphore_signal(
            barrier, inc=1, device_id={"fs": (f + k) % n_fs}, device_id_type=MESH
        )

    @pl.loop(1, n_tp)
    def _(k):
        pl.semaphore_signal(
            barrier, inc=1, device_id={"tp": (t + k) % n_tp}, device_id_type=MESH
        )

    loads[4].wait()
    loads[5].wait()
    names = lax.broadcasted_iota(jnp.int32, (n_fs, tok), 0)
    chosen = jnp.zeros((n_fs, tok), F32)
    weight = jnp.zeros((n_fs, tok), F32)
    for k in range(experts_ref.shape[0]):
        hit = experts_ref[k : k + 1, :] == names
        chosen = chosen + jnp.where(hit, 1.0, 0.0)
        weight = weight + jnp.where(hit, routing_ref[k : k + 1, :], 0.0)
    before = jnp.where(
        lax.broadcasted_iota(jnp.int32, (tok, tok), 0)
        < lax.broadcasted_iota(jnp.int32, (tok, tok), 1),
        1.0,
        0.0,
    ).astype(BF)
    rank = jnp.dot(chosen.astype(BF), before, preferred_element_type=F32)
    slot_v[...] = jnp.where(chosen > 0.0, rank, -1.0)
    weight_v[...] = weight
    places = lax.broadcasted_iota(jnp.int32, (cap, tok), 0).astype(F32)

    @pl.loop(0, n_fs)
    def _(e):
        hit = slot_v[pl.ds(e, 1), :] == places
        at = pl.ds(pl.multiple_of(e * cap, 8), cap)
        pick_v[at, :] = jnp.where(hit, 1.0, 0.0)

    loads[0].wait()
    sent = jnp.dot(pick_v[...].astype(BF), tok_v[...], preferred_element_type=F32)
    t_send[...] = sent.astype(BF).reshape(tiles, 8, fcols)

    loads[6].wait()
    here = lax.broadcasted_iota(jnp.int32, (stripe, hid), 0) + (f * stripe) % hid
    lane = lax.broadcasted_iota(jnp.int32, (stripe, hid), 1)
    picked = jnp.where(here == lane, gain_ref[pl.ds((f * stripe) // hid, 1), :], 0.0)
    column = jnp.sum(picked, axis=1, keepdims=True)
    loads[1].wait()
    loads[2].wait()

    @pl.loop(0, n_fs)
    def _(e):
        w_send[e, :, 0:hid] = (gate_v[e] * column).astype(BF)
        w_send[e, :, hid : 2 * hid] = (linear_v[e] * column).astype(BF)

    loads[3].wait()
    pl.semaphore_wait(barrier, n_fs + n_tp - 2)

    def tile_span(i):
        return pl.ds(i * per, per)

    def peer(dz, dc):
        return ((z + dz) % n_z) * 2 + (c + dc) % 2

    def turn(k):
        return (n_z // 2 + (1 - 2 * (k % 2)) * ((k + 1) // 2)) % n_z

    def tokens_copy(k, to, slot, count=1):
        return remote(
            t_send.at[pl.ds(to * per, count * per)],
            t_grid.at[t, pl.ds(slot * per, count * per)],
            t_ssem.at[0],
            t_rsem.at[0],
            {"fs": to if count == 1 else (f + 1) % n_fs},
        )

    def weights_copy(k, to, slot, count=1):
        i = (k + 1) // 2
        src, dst = w_send.at[pl.ds(to, count)], w_recv.at[pl.ds(slot, count)]
        device = to if count == 1 else (f + 1) % n_fs
        return remote(src, dst, w_ssem.at[0], w_rsem.at[i], {"fs": device})

    def start_all(copy, core):
        dc = (core + c) % 2

        @pl.loop(0, n_z - 1)
        def _(k):
            copy(k, peer(turn(k), dc), f).start()

        @pl.when(dc == 1)
        def _():
            copy(n_z - 1, peer(0, 1), f).start()

    def down_y(k, slot):
        to = (y + k) % SIDE
        return remote(
            down_v.at[to], d_grid.at[slot, x], dy_ssem.at[0], dy_rsem.at[k], {"tp": to * SIDE + x}
        )

    def down_ref(p, k, part):
        block = d_grid.at[(y - k + SIDE) % SIDE, p]
        half = d_grid.shape[2] // 2
        return block if part is None else block.at[pl.ds(part * half, half)]

    dx = Ring(down_ref, lambda p: {"tp": y * SIDE + p}, dx_ssem, dx_rsem, x)

    start_all(tokens_copy, 0)
    start_all(tokens_copy, 1)
    start_all(weights_copy, 0)
    start_all(weights_copy, 1)

    for k in (1, 3, 2):
        down_y(k, y).start()
    d_grid[y, x] = down_v[y]
    dx.first(0)

    t_grid[t, tile_span(f)] = t_send[tile_span(f)]
    w_recv[f] = w_send[f]
    @pl.loop(0, n_fs)
    def _(e):
        hit = slot_v[pl.ds(e, 1), :] == places
        at = pl.ds(pl.multiple_of(e * cap, 8), cap)
        mixer_v[at, :] = jnp.where(hit, weight_v[pl.ds(e, 1), :], 0.0)

    for j in range(rows // 128):
        at = slice(j * 128, (j + 1) * 128)
        turned = mixer_v[at, :].T
        high = turned.astype(BF)
        high_v[:, at] = high
        low_v[:, at] = (turned - high.astype(F32)).astype(BF)
    acc[...] = jnp.zeros_like(acc)

    for k in (1, 3, 2):
        down_y(k, (y - k + SIDE) % SIDE).wait_recv()
        dx.first(k)

    tokens_copy(0, 0, 0, n_fs - 1).wait_recv()
    tg = Torus(t_grid, tg_ssem, tg_rsem, t)
    tg.own()
    for k in (0, 1, 3, 2):
        dx.second(k)
    tg.rest()
    dx.whole(d_grid.at[0]).wait_recv()

    @pl.loop(0, n_tp)
    def _(b):
        t_rows[b] = t_grid[b].reshape(rows, fcols)

    @pl.loop(0, SIDE)
    def _(p):
        for g in range(SIDE):
            d_turned[p, g * hid : (g + 1) * hid, :] = d_grid[p, g].T


    def lhs(chip):
        return t_rows[chip]

    def rhs(chip):
        return w_recv[pl.ds(chip * 2, 2)].reshape(fcols, 2 * hid)

    def multiply(one, other):
        acc[...] += jnp.dot(
            jnp.concatenate([lhs(one), lhs(other)], axis=1),
            jnp.concatenate([rhs(one), rhs(other)], axis=0),
            preferred_element_type=F32,
        )

    weights_copy(n_z - 1, peer(0, 1), peer(0, 1)).wait_recv()
    weights_copy(0, 0, 0, 2).wait_recv()
    multiply(z, (z + n_z // 2) % n_z)

    @pl.loop(1, n_z // 2)
    def _(k):
        weights_copy(2 * k, 0, 0, 4).wait_recv()
        multiply((z + n_z // 2 + k) % n_z, (z + n_z // 2 - k) % n_z)

    n_q = a_send.shape[0]
    offsets = (4, 5, 3, 6, 2, 1, 7, 0)
    chunk = n_q // CHUNKS
    span = rows // n_q
    groups = (1, 3, 2)
    others = sorted(
        ((a, b) for a in range(SIDE) for b in range(SIDE) if (a, b) != (0, 0)),
        key=lambda ab: -min(ab[0], SIDE - ab[0]) - min(ab[1], SIDE - ab[1]),
    )

    def q_of(j):
        return (z // 2 + offsets[j]) % n_q

    def active_copy(r, to):
        return remote(
            a_send.at[pl.ds(r * chunk, chunk), to % SIDE],
            a_grid.at[t, pl.ds(r * chunk, chunk)],
            a_ssem.at[0],
            a_rsem.at[r],
            {"tp": to},
        )

    def ahead(dy_, dx_):
        return (y + dy_) % SIDE * SIDE + (x + dx_) % SIDE

    def arrived(at):
        ref = a_grid.at[pl.ds(0, n_tp - 1), at]
        return lambda r: remote(ref, ref, a_ssem.at[0], a_rsem.at[r], {"tp": ahead(0, 1)})

    for r in range(CHUNKS):
        for j in range(r * chunk, (r + 1) * chunk):
            at = pl.ds(pl.multiple_of(q_of(j) * span, 8), span)
            clamped = jnp.minimum(acc[at, 0:hid], clamp_limit)
            linear = jnp.clip(acc[at, hid : 2 * hid], -clamp_limit, clamp_limit)
            active = clamped * jax.nn.sigmoid(gate_slope * clamped) * (linear + 1.0)
            a_send[j] = active.astype(BF).reshape(a_send.shape[1:])
        for dy_, dx_ in others:
            active_copy(r, ahead(dy_, dx_)).start()
    a_grid[t] = a_send[:, x]
    stores = [
        pltpu.make_async_copy(w_recv.at[:, :, pl.ds(0, hid)], gate_out, local_sems.at[7]),
        pltpu.make_async_copy(w_recv.at[:, :, pl.ds(hid, hid)], linear_out, local_sems.at[8]),
    ]
    for store in stores:
        store.start()

    share = chunk * span // SIDE

    def multiply_down(r):
        at = pl.ds(r * chunk, chunk)
        total = jnp.zeros((share, d_turned.shape[2]), F32)
        for p in range(SIDE):
            total = total + lax.dot_general(
                jnp.concatenate(
                    [a_grid[p * SIDE + g, at].reshape(share, hid) for g in range(SIDE)], axis=1
                ),
                d_turned[p],
                (((1,), (0,)), ((), ())),
                preferred_element_type=F32,
            )
        return total

    def return_copy(j, p):
        to = q_of(j) * SIDE + x
        return remote(
            r_send.at[p, j],
            r_recv.at[f],
            r_ssem.at[0],
            r_rsem.at[0],
            {"fs": to, "tp": y * SIDE + p},
        ), jnp.logical_and(to == f, p == x)

    def each_return(r, act):
        for j in range(r * chunk, (r + 1) * chunk):
            for p in range(SIDE):
                c, local = return_copy(j, p)
                if offsets[j] != 0:
                    act(c)
                else:

                    @pl.when(jnp.logical_not(local))
                    def _():
                        act(c)

    weights_copy(0, 0, 0, n_fs - 1).wait_send()
    for r in range(CHUNKS):
        arrived(pl.ds(0, chunk))(r).wait_recv()
        total = multiply_down(r)
        for p in range(SIDE):
            part = total[:, p * fcols : (p + 1) * fcols].astype(BF)
            r_send[p, pl.ds(r * chunk, chunk)] = part.reshape(chunk, *r_send.shape[2:])
        each_return(r, lambda c: c.start())

    @pl.when(f % SIDE == x)
    def _():
        r_recv[f] = r_send[x, offsets.index(0)]

    tokens_copy(0, 0, 0, n_fs - 1).wait_send()
    remote(
        down_v.at[pl.ds(1, SIDE - 1)],
        d_grid.at[0, pl.ds(1, SIDE - 1)],
        dy_ssem.at[0],
        dy_rsem.at[1],
        {"tp": ahead(1, 0)},
    ).wait_send()
    dx.whole(d_grid.at[pl.ds(0, SIDE - 1)]).wait_send()
    tg.drain()
    arrived(pl.ds(0, n_q))(0).wait_send()
    for store in stores:
        store.wait()

    def returned(count):
        ref = r_recv.at[pl.ds(0, count)]
        return remote(ref, ref, r_ssem.at[0], r_rsem.at[0], {"fs": (f + 1) % n_fs})

    mine = f % SIDE == x

    @pl.when(mine)
    def _():
        returned(n_fs - 1).wait_recv()

    @pl.when(jnp.logical_not(mine))
    def _():
        returned(n_fs).wait_recv()

    back = r_recv[...].reshape(rows, fcols)
    mix = jnp.dot(high_v[...], back, preferred_element_type=F32) + jnp.dot(
        low_v[...], back, preferred_element_type=F32
    )
    mix_out[...] = mix.astype(BF)

    @pl.when(mine)
    def _():
        returned(n_fs - 1).wait_send()

    @pl.when(jnp.logical_not(mine))
    def _():
        returned(n_fs).wait_send()


def copy_out(a, b, c, a_out, b_out, c_out, sems):
    copies = [
        pltpu.make_async_copy(src, dst, sems.at[i])
        for i, (src, dst) in enumerate(((a, a_out), (b, b_out), (c, c_out)))
    ]
    for copy in copies:
        copy.start()
    for copy in copies:
        copy.wait()


def on_device(n_fs, n_tp, tokens, experts, routing, gain, gate_master, linear_master, down_weight):
    tok, top = experts.shape
    ecount, stripe, hid = gate_master.shape
    width = tokens.shape[1]
    fcols = width // n_tp
    cap = 3 * tok * top // (2 * ecount)
    tiles = ecount * cap // 8
    rows = ecount * cap
    vmem, any_space = pl.BlockSpec(memory_space=pltpu.VMEM), pl.BlockSpec(memory_space=pl.ANY)
    hbm = pl.BlockSpec(memory_space=pltpu.HBM)
    sources = ecount // SIDE
    dma = pltpu.SemaphoreType.DMA
    gate_out, linear_out, mix = pl.pallas_call(
        functools.partial(kernel, n_fs, n_tp),
        out_shape=(
            jax.ShapeDtypeStruct((ecount, stripe, hid), BF),
            jax.ShapeDtypeStruct((ecount, stripe, hid), BF),
            jax.ShapeDtypeStruct((tok, fcols), BF),
        ),
        in_specs=[hbm] * 7,
        out_specs=(any_space, any_space, vmem),
        scratch_shapes=[
            pltpu.VMEM((top, tok), jnp.int32),
            pltpu.VMEM((top, tok), F32),
            pltpu.VMEM((width // hid, hid), F32),
            pltpu.VMEM((ecount, stripe, hid), F32),
            pltpu.VMEM((ecount, stripe, hid), F32),
            pltpu.VMEM((tok, fcols), BF),
            pltpu.VMEM((SIDE, width // SIDE, hid), BF),
            pltpu.VMEM((ecount, stripe, 2 * hid), BF),
            pltpu.VMEM((ecount, stripe, 2 * hid), BF),
            pltpu.VMEM((tiles, 8, fcols), BF),
            pltpu.VMEM((n_tp, tiles, 8, fcols), BF),
            pltpu.VMEM((n_tp, rows, fcols), BF),
            pltpu.VMEM((sources, SIDE, cap // 8, 8, hid), BF),
            pltpu.VMEM((n_tp, sources, cap // 8, 8, hid), BF),
            pltpu.VMEM((SIDE, SIDE, width // SIDE, hid), BF),
            pltpu.VMEM((SIDE, SIDE * hid, width // SIDE), BF),
            pltpu.VMEM((SIDE, sources, cap // 8, 8, fcols), BF),
            pltpu.VMEM((ecount, cap // 8, 8, fcols), BF),
            pltpu.VMEM((ecount, tok), F32),
            pltpu.VMEM((ecount, tok), F32),
            pltpu.VMEM((rows, tok), F32),
            pltpu.VMEM((rows, tok), F32),
            pltpu.VMEM((tok, rows), BF),
            pltpu.VMEM((tok, rows), BF),
            pltpu.VMEM((rows, 2 * hid), F32),
            dma((9,)),
            dma((1,)),
            dma((1,)),
            dma((1,)),
            dma((ecount // 4 + 1,)),
            dma((1,)),
            dma((1,)),
            dma((1,)),
            dma((SIDE,)),
            dma((1,)),
            dma((9,)),
            dma((1,)),
            dma((25,)),
            dma((1,)),
            dma((CHUNKS,)),
        ],
        compiler_params=pltpu.CompilerParams(
            collective_id=0, has_side_effects=True, vmem_limit_bytes=48 * 1024 * 1024
        ),
    )(
        *[
            pltpu.with_memory_space_constraint(v, pltpu.HBM)
            for v in (
                experts.T,
                routing.T,
                gain.reshape(width // hid, hid),
                tokens,
                gate_master,
                linear_master,
                down_weight.reshape(SIDE, width // SIDE, hid),
            )
        ]
    )
    shape = (1, width, hid)
    results = (gate_out.reshape(shape), linear_out.reshape(shape), mix)
    return pl.pallas_call(
        copy_out,
        out_shape=tuple(jax.ShapeDtypeStruct(v.shape, v.dtype) for v in results),
        in_specs=[vmem] * 3,
        out_specs=(hbm,) * 3,
        scratch_shapes=[dma((3,))],
    )(*[pltpu.with_memory_space_constraint(v, pltpu.VMEM) for v in results])


def solution(mesh):
    n_fs, n_tp = mesh.shape["fs"], mesh.shape["tp"]
    return jax.shard_map(
        functools.partial(on_device, n_fs, n_tp),
        mesh=mesh,
        in_specs=(
            P("fs", None),
            P("fs", None),
            P("fs", None),
            P(),
            P(None, "fs", "tp"),
            P(None, "fs", "tp"),
            P("fs", None, "tp"),
        ),
        out_specs=(P("fs", None, "tp"), P("fs", None, "tp"), P("fs", "tp")),
        check_vma=False,
    )
```
